32 devices in a mesh: ep: 16 (over z, y, x), tp: 2 (over core).
Axes of the slice: x: 2, y: 2, z: 4, core: 2. Of those that a mesh axis runs over, the one named last changes fastest.
Arguments:
- tokens: bfloat16 [256, 2048], P('ep'), may hold values from -6 to 6
- norm_attn: float32 [2048], replicated, may hold values from 0.1 to 1.9
- w_query: bfloat16 [2048, 2048], P(None, 'tp'), may hold values from -0.125 to 0.125
- w_key: bfloat16 [2048, 256], P(None, 'tp'), may hold values from -0.125 to 0.125
- w_value: bfloat16 [2048, 256], P(None, 'tp'), may hold values from -0.125 to 0.125
- w_out: bfloat16 [2048, 2048], P('tp'), may hold values from -0.125 to 0.125
- attn_bias: float32 [32], P('tp'), may hold values from -7 to -1
- cache_keys: bfloat16 [256, 1024, 256], P('ep', None, 'tp'), may hold values from -6 to 6
- cache_values: bfloat16 [256, 1024, 256], P('ep', None, 'tp'), may hold values from -6 to 6
- lengths: int32 [256], P('ep'), may hold values from 256 to 1024
- norm_ffn: float32 [2048], replicated, may hold values from 0.1 to 1.9
- expert_gate: bfloat16 [2048, 57344], P(None, ('ep', 'tp')), may hold values from -0.125 to 0.125
- expert_up: bfloat16 [2048, 57344], P(None, ('ep', 'tp')), may hold values from -0.125 to 0.125
- expert_down: bfloat16 [57344, 2048], P(('ep', 'tp')), may hold values from -0.0625 to 0.0625
- dense_gate_w: bfloat16 [2048, 7168], P(None, 'ep'), may hold values from -0.125 to 0.125
- dense_up_w: bfloat16 [2048, 7168], P(None, 'ep'), may hold values from -0.125 to 0.125
- dense_down_w: bfloat16 [7168, 2048], P('ep'), may hold values from -0.0625 to 0.0625
- dense_mix: bfloat16 [2048], replicated, may hold values from -0.125 to 0.125
- routes: int32 [256, 2], P(('ep', 'tp')), may hold values from 0 to 7, all different within a row; in each aligned block of 8 rows (0 to 7, 8 to 15, ...) at most 3 rows name the same one
- route_weights: bfloat16 [256, 2], P(('ep', 'tp')), may hold values from 0.19921875 to 1
Outputs:
- layer_out: bfloat16 [256, 2048], P(('ep', 'tp'))
- new_keys: bfloat16 [256, 256], P('ep', 'tp')
- new_values: bfloat16 [256, 256], P('ep', 'tp')
The draws below stay inside these ranges and needn't reach their ends.
Inputs may be any that keep to these rules, and one draw needn't show every extreme that they name: `routes`: in each aligned block of 8 rows (the rows of one device) no expert is named by more than 3 rows, a bound that some block reaches; a row names 2 different experts.
All inputs are finite; a program needn't handle non-finite values.
Results may differ from the reference program's by a relative error of at most 0.015.
Values may be sent and summed in bfloat16 or wider, within the bound.
No kernel may reach another device: no remote copies, remote signals or barrier semaphores. Data moves between devices by JAX's collectives and lax.ppermute only.
A program may use at most 128 MiB of HBM per device.

```python
import math
import jax
import jax.numpy as jnp
import numpy as np
from jax import lax

D = 2048
HEADS = 32
KV_HEADS = 4
HEAD_DIM = 64
FF = 7168
DENSE_FF = 7168
EXPERTS = 8
TOP = 2
SEQS_DEV = 16
CACHE = 1024
TOKENS = 256
ROWS_DEV = 8
CAP_DEV = 3
N_EP = 16
N_TP = 2


def place_ends(drawn, key, low, largest):
    dims = drawn.shape
    spot = [jax.random.randint(jax.random.fold_in(key, axis), (), 0, dims[axis]) for axis in range(len(dims))]
    drawn = drawn.at[tuple(spot)].set(low)
    longest = dims.index(max(dims))
    spot[longest] = (spot[longest] + 1) % dims[longest]
    return drawn.at[tuple(spot)].set(largest)


def steps_of(own_key, dims, pieces, smallest, top_value):
    def one(position, blocks):
        steps = jax.random.uniform(jax.random.fold_in(jax.random.fold_in(own_key, 6), position), (blocks,), jnp.float32, smallest / len(pieces), top_value / len(pieces))
        return jnp.repeat(jnp.exp(steps), dims[position] // blocks).reshape((-1,) + (1,) * (len(dims) - position - 1))

    level = one(*pieces[0])
    for cut in pieces[1:]:
        level = level * one(*cut)
    return level


def assign_block(key, own, number, rows, count, top, limit, lean):
    sequence = jax.random.permutation(key, count)
    crowded, ordinary = portions_of(count, rows * top, limit, lean, True), portions_of(count, rows * top, limit, lean, False)
    places = jnp.arange(count)

    def named(tallies, rotation):
        used = int((tallies > 0).sum())
        fixed = max(1, used // 4)
        moved = fixed + (places - fixed + rotation * (used - fixed)) % max(1, count - fixed)
        return jnp.zeros((count,), jnp.int32).at[sequence[jnp.where(places < fixed, places, moved)]].set(jnp.asarray(tallies, jnp.int32))

    tallies = jnp.where(number % 4 == 0, named(crowded, number // 4), named(ordinary, number - number // 4 - 1))
    mixed = jax.random.permutation(jax.random.fold_in(own, 3), count)
    source_of, sink = mixed[0:count // 2 * 2:2], mixed[1:count // 2 * 2:2]
    margin = jnp.minimum(tallies[source_of] - 1, limit - tallies[sink]) // 2
    margin = jnp.where((source_of == sequence[0]) | (sink == sequence[0]) | (tallies[sink] == 0), 0, jnp.maximum(margin, 0))
    moved = jax.random.randint(jax.random.fold_in(own, 4), (count // 2,), 0, 1 << 20) % (margin + 1)
    tallies = tallies.at[source_of].add(-moved).at[sink].add(moved)
    members = jnp.searchsorted(jnp.cumsum(tallies), jnp.arange(rows * top), side="right").astype(jnp.int32)
    grid = members.reshape(top, rows).T
    grid = grid[jax.random.permutation(jax.random.fold_in(own, 1), rows)]
    rotation = jax.random.randint(jax.random.fold_in(own, 2), (rows, 1), 0, top)
    return jnp.take_along_axis(grid, (jnp.arange(top)[None, :] + rotation) % top, axis=1)


def portions_of(amount, total, reach, slope, full):
    weights = [(1 << 20) // math.isqrt(grade ** slope) + 1 for grade in range(1, amount + 1)]
    largest = reach if full else min(reach, max(-(-total // amount), total * weights[0] // sum(weights)))
    least = 1 if total - largest >= amount - 1 else 0
    given, surplus = [largest] + [least] * (amount - 1), total - largest - least * (amount - 1)
    while surplus > 0:
        free = [i for i in range(1, amount) if given[i] < largest] or [i for i in range(1, amount) if given[i] < reach]
        whole, budget = sum([weights[i] for i in free]), surplus
        for i in free:
            extra = min(reach - given[i], max(1, budget * weights[i] // whole), surplus)
            given[i] = given[i] + extra
            surplus = surplus - extra
    return np.array(given)


def scatter_about(key, dims, deviation, bound, cuts=(), kind=jnp.bfloat16):
    drawn = deviation * jax.random.normal(key, dims, jnp.float32)
    if cuts:
        drawn = drawn * steps_of(key, dims, cuts, -0.22, 0.18)
    return jnp.clip(drawn, -bound, bound).astype(kind)


def setup_inputs(seed: int = 0) -> dict:
    key_of = jax.random.split(jax.random.key(seed), 21)
    tokens = scatter_about(key_of[0], (TOKENS, D), 1.0, 6.0, ((0, 16),))
    norm_attn = jnp.clip(1.0 + 0.18 * jax.random.normal(key_of[1], (D,), jnp.float32), 0.1, 1.9)
    w_query = scatter_about(key_of[2], (D, HEADS * HEAD_DIM), D ** -0.5, 0.125, ((1, 2),))
    w_key = scatter_about(key_of[3], (D, KV_HEADS * HEAD_DIM), D ** -0.5, 0.125, ((1, 2),))
    w_value = scatter_about(key_of[4], (D, KV_HEADS * HEAD_DIM), D ** -0.5, 0.125, ((1, 2),))
    w_out = scatter_about(key_of[5], (HEADS * HEAD_DIM, D), (HEADS * HEAD_DIM) ** -0.5, 0.125, ((0, 2),))
    attn_bias = jnp.clip(-7.0 + 6.0 * jax.random.uniform(key_of[6], (HEADS,), jnp.float32) ** steps_of(key_of[6], (HEADS,), ((0, 2),), -0.2, 0.2), -7.0, -1.0)
    cache_keys = scatter_about(key_of[7], (TOKENS, CACHE, KV_HEADS * HEAD_DIM), 1.0, 6.0, ((0, 16), (2, 2)))
    cache_values = scatter_about(key_of[8], (TOKENS, CACHE, KV_HEADS * HEAD_DIM), 1.0, 6.0, ((0, 16), (2, 2)))
    lengths = place_ends(jax.random.randint(key_of[9], (TOKENS,), CACHE // 4, CACHE + 1), jax.random.fold_in(key_of[9], 1), CACHE // 4, CACHE).astype(jnp.int32)
    norm_ffn = jnp.clip(1.0 + 0.18 * jax.random.normal(key_of[10], (D,), jnp.float32), 0.1, 1.9)
    expert_gate = scatter_about(key_of[11], (D, EXPERTS * FF), D ** -0.5, 0.125, ((1, 32),))
    expert_up = scatter_about(key_of[12], (D, EXPERTS * FF), D ** -0.5, 0.125, ((1, 32),))
    expert_down = scatter_about(key_of[13], (EXPERTS * FF, D), FF ** -0.5, 0.0625, ((0, 32),))
    dense_gate_w = scatter_about(key_of[14], (D, DENSE_FF), D ** -0.5, 0.125, ((1, 16),))
    dense_up_w = scatter_about(key_of[15], (D, DENSE_FF), D ** -0.5, 0.125, ((1, 16),))
    dense_down_w = scatter_about(key_of[16], (DENSE_FF, D), DENSE_FF ** -0.5, 0.0625, ((0, 16),))
    dense_mix = scatter_about(key_of[17], (D,), D ** -0.5, 0.125)
    routes_keys = jax.random.split(jax.random.fold_in(key_of[18], 1), TOKENS // ROWS_DEV)
    routes_turns = jax.random.permutation(jax.random.fold_in(key_of[18], 3), TOKENS // ROWS_DEV)
    routes = jax.vmap(lambda own, number: assign_block(jax.random.fold_in(key_of[18], 2), own, number, ROWS_DEV, EXPERTS, TOP, CAP_DEV, 1))(routes_keys, routes_turns).reshape((TOKENS, TOP))
    route_weights = jnp.clip(jnp.exp(math.log(1.0) - 1.6133518 * jax.random.uniform(key_of[19], (TOKENS, TOP), jnp.float32) ** steps_of(key_of[19], (TOKENS, TOP), ((0, 32),), -0.2, 0.2)), 0.19921875, 1.0).astype(jnp.bfloat16)
    return {"tokens": tokens, "norm_attn": norm_attn, "w_query": w_query, "w_key": w_key, "w_value": w_value, "w_out": w_out, "attn_bias": attn_bias, "cache_keys": cache_keys, "cache_values": cache_values, "lengths": lengths, "norm_ffn": norm_ffn, "expert_gate": expert_gate, "expert_up": expert_up, "expert_down": expert_down, "dense_gate_w": dense_gate_w, "dense_up_w": dense_up_w, "dense_down_w": dense_down_w, "dense_mix": dense_mix, "routes": routes, "route_weights": route_weights}


EPSILON = 1e-06

def normed_rows(values, gain):
    widened = values.astype(jnp.float32)
    scale = lax.rsqrt(lax.optimization_barrier(jnp.mean(widened * widened, axis=-1, keepdims=True)) + EPSILON)
    return (widened * scale * gain).astype(jnp.bfloat16)

def reference(tokens, norm_attn, w_query, w_key, w_value, w_out, attn_bias, cache_keys, cache_values, lengths, norm_ffn, expert_gate, expert_up, expert_down, dense_gate_w, dense_up_w, dense_down_w, dense_mix, routes, route_weights):
    repeat = HEADS // KV_HEADS
    normed = normed_rows(tokens, norm_attn)
    query = jnp.dot(normed, w_query, preferred_element_type=jnp.float32).astype(jnp.bfloat16)
    new_keys = jnp.dot(normed, w_key, preferred_element_type=jnp.float32).astype(jnp.bfloat16)
    new_values = jnp.dot(normed, w_value, preferred_element_type=jnp.float32).astype(jnp.bfloat16)
    offsets = attn_bias.reshape(KV_HEADS, repeat)

    def attend(block):
        query_block, key_block, value_block, length_block = block
        query_heads = query_block.astype(jnp.float32).reshape(SEQS_DEV, KV_HEADS, repeat, HEAD_DIM)
        key_heads = key_block.astype(jnp.float32).reshape(SEQS_DEV, CACHE, KV_HEADS, HEAD_DIM)
        value_heads = value_block.astype(jnp.float32).reshape(SEQS_DEV, CACHE, KV_HEADS, HEAD_DIM)
        scores = jnp.einsum('bgrd,bsgd->bgrs', query_heads, key_heads) * HEAD_DIM ** (-0.5)
        scores = scores + offsets[None, :, :, None]
        places = lax.broadcasted_iota(jnp.int32, (SEQS_DEV, CACHE), 1)
        visible = (places < length_block[:, None])[:, None, None, :]
        log_keep = jnp.where(visible, jax.nn.log_sigmoid(-scores), 0.0)
        after = lax.cumsum(log_keep, axis=3, reverse=True) - log_keep
        weight = jnp.where(visible, jnp.exp(jax.nn.log_sigmoid(scores) + after), 0.0).astype(jnp.bfloat16)
        mixed = jnp.einsum('bgrs,bsgd->bgrd', weight.astype(jnp.float32), value_heads)
        return mixed.astype(jnp.bfloat16).reshape(SEQS_DEV, HEADS * HEAD_DIM)
    heads_out = lax.map(attend, (query.reshape(N_EP, SEQS_DEV, HEADS * HEAD_DIM), cache_keys.reshape(N_EP, SEQS_DEV, CACHE, KV_HEADS * HEAD_DIM), cache_values.reshape(N_EP, SEQS_DEV, CACHE, KV_HEADS * HEAD_DIM), lengths.reshape(N_EP, SEQS_DEV))).reshape(TOKENS, HEADS * HEAD_DIM)
    run_width = HEADS * HEAD_DIM // N_TP
    attn_sum = jnp.zeros((TOKENS, D), jnp.float32)
    for run in range(N_TP):
        partial_value = jnp.dot(heads_out[:, run * run_width:(run + 1) * run_width], w_out[run * run_width:(run + 1) * run_width], preferred_element_type=jnp.float32)
        attn_sum = attn_sum + lax.optimization_barrier(partial_value.astype(jnp.bfloat16)).astype(jnp.float32)
    middle = (tokens.astype(jnp.float32) + attn_sum).astype(jnp.bfloat16)
    normed_two = normed_rows(middle, norm_ffn)
    mix_gate = jax.nn.sigmoid(jnp.dot(normed_two, dense_mix, preferred_element_type=jnp.float32))
    dense_hidden = (jax.nn.silu(jnp.dot(normed_two, dense_gate_w, preferred_element_type=jnp.float32)) * jnp.dot(normed_two, dense_up_w, preferred_element_type=jnp.float32)).astype(jnp.bfloat16)
    dense_term = jnp.dot(dense_hidden, dense_down_w, preferred_element_type=jnp.float32) * mix_gate[:, None]
    sources = N_EP * N_TP
    route_blocks = routes.reshape(sources, ROWS_DEV, TOP)
    weight_blocks = route_weights.astype(jnp.float32).reshape(sources, ROWS_DEV, TOP)
    row_blocks = normed_two.astype(jnp.float32).reshape(sources, ROWS_DEV, D)
    slot_ids = lax.broadcasted_iota(jnp.int32, (sources, CAP_DEV, ROWS_DEV), 1)

    def one_expert(expert_id):
        matched = route_blocks == expert_id
        present = jnp.any(matched, axis=2).astype(jnp.int32)
        share = lax.optimization_barrier(jnp.sum(jnp.where(matched, weight_blocks, 0.0), axis=2))
        ranks = jnp.cumsum(present, axis=1) - 1
        selector = ((present[:, None, :] == 1) & (ranks[:, None, :] == slot_ids)).astype(jnp.float32)
        slot_rows = jnp.einsum('dcr,drk->dck', selector, row_blocks).astype(jnp.bfloat16).reshape(sources * CAP_DEV, D)
        start = (expert_id * FF).astype(jnp.int32)
        gate_cols = lax.dynamic_slice_in_dim(expert_gate, start, FF, 1)
        up_cols = lax.dynamic_slice_in_dim(expert_up, start, FF, 1)
        down_rows = lax.dynamic_slice_in_dim(expert_down, start, FF, 0)
        hidden = (jax.nn.silu(jnp.dot(slot_rows, gate_cols, preferred_element_type=jnp.float32)) * jnp.dot(slot_rows, up_cols, preferred_element_type=jnp.float32)).astype(jnp.bfloat16)
        result = jnp.dot(hidden, down_rows, preferred_element_type=jnp.float32).reshape(sources, CAP_DEV, D)
        returned = jnp.einsum('dcr,dck->drk', selector, result) * share[:, :, None]
        return returned.reshape(TOKENS, D)
    expert_term = lax.optimization_barrier(jnp.sum(lax.map(one_expert, jnp.arange(EXPERTS, dtype=jnp.int32)), axis=0))
    layer_out = (middle.astype(jnp.float32) + expert_term + dense_term).astype(jnp.bfloat16)
    return (layer_out, new_keys, new_values)
```

```python
import functools

import jax
import jax.numpy as jnp
from jax import lax
from jax.experimental import pallas as pl
from jax.experimental.pallas import tpu as pltpu
from jax.sharding import PartitionSpec as P

HEAD_DIM = 64
EXPERTS = 8
LANES = 128
EPSILON = 1e-06
F32 = jnp.float32
BF16 = jnp.bfloat16


ANY = pl.BlockSpec(memory_space=pl.ANY)
VMEM = pl.BlockSpec(memory_space=pltpu.VMEM)
SMEM = pl.BlockSpec(memory_space=pltpu.SMEM)


def split_of(total, most):
    for pieces in range(most, 0, -1):
        if total % (pieces * 256) == 0:
            return pieces
    return 1


def normed_block(widened, gain):
    scale = lax.rsqrt(jnp.mean(widened * widened, axis=-1, keepdims=True) + EPSILON)
    return (widened * scale * gain).astype(BF16)


def attention_kernel(
    row_count, group,
    lengths_ref, tokens_ref, gain_ref, bias_ref,
    wq_hbm, wk_hbm, wv_hbm, wo_hbm, keys_hbm, values_hbm,
    keep_ref, send_ref, new_keys_ref, new_values_ref,
    wq, wk, wv, wo, keys, values, queries, mixed, later, partial,
    sem_q, sem_kv, sem_k, sem_v, sem_o,
):
    seqs, width = tokens_ref.shape
    cache = keys.shape[1]
    q_width = wq.shape[1]
    heads = q_width // HEAD_DIM
    pairs = heads // 2
    q_parts = sem_q.shape[0]
    o_parts = sem_o.shape[0]
    groups = seqs // group
    q_rows = width // q_parts
    o_rows = q_width // o_parts
    half = 2 * LANES

    def q_copy(i):
        rows = pl.ds(i * q_rows, q_rows)
        return pltpu.make_async_copy(wq_hbm.at[rows], wq.at[rows], sem_q.at[i])

    def o_copy(i):
        rows = pl.ds(i * o_rows, o_rows)
        return pltpu.make_async_copy(wo_hbm.at[rows], wo.at[rows], sem_o.at[i])

    def k_copy(i):
        rows = pl.ds(i * group, group)
        return pltpu.make_async_copy(keys_hbm.at[rows], keys.at[rows], sem_k.at[i])

    def v_copy(i):
        rows = pl.ds(i * group, group)
        return pltpu.make_async_copy(values_hbm.at[rows], values.at[rows], sem_v.at[i])

    copy_wk = pltpu.make_async_copy(wk_hbm, wk, sem_kv.at[0])
    copy_wv = pltpu.make_async_copy(wv_hbm, wv, sem_kv.at[1])
    for i in range(q_parts):
        q_copy(i).start()
    for i in range(groups):
        k_copy(i).start()
        v_copy(i).start()
    copy_wk.start()
    copy_wv.start()
    for i in range(o_parts):
        o_copy(i).start()

    later_rows = lax.broadcasted_iota(jnp.int32, (2 * half, half), 0) % half
    later_cols = lax.broadcasted_iota(jnp.int32, (2 * half, half), 1)
    later[...] = (later_rows > later_cols).astype(F32).astype(BF16)

    normed = normed_block(tokens_ref[...].astype(F32), gain_ref[...])
    query = jnp.zeros((seqs, q_width), F32)
    for i in range(q_parts):
        q_copy(i).wait()
        query += jnp.dot(
            normed[:, i * q_rows:(i + 1) * q_rows],
            wq[i * q_rows:(i + 1) * q_rows, :],
            preferred_element_type=F32,
        )
    query = query.astype(BF16).astype(F32)

    lane = lax.broadcasted_iota(jnp.int32, (seqs, LANES), 1)
    low = lane < HEAD_DIM
    for pair in range(pairs):
        both = query[:, pair * LANES:(pair + 1) * LANES]
        turned = pltpu.roll(both, HEAD_DIM, 1)
        if 2 * pair < heads // 2:
            first, second = jnp.where(low, both, 0.0), jnp.where(low, turned, 0.0)
        else:
            first, second = jnp.where(low, 0.0, turned), jnp.where(low, 0.0, both)
        queries[pl.ds(2 * pair, seqs, stride=heads), :] = first
        queries[pl.ds(2 * pair + 1, seqs, stride=heads), :] = second

    rows = group * heads
    head_of = lax.broadcasted_iota(jnp.int32, (heads, 1), 0)
    bias = jnp.zeros((heads, 1), F32)
    for head in range(heads):
        bias = jnp.where(head_of == head, bias_ref[head], bias)
    bias = jnp.concatenate([bias] * group, axis=0)
    seq_of = lax.broadcasted_iota(jnp.int32, (rows, 1), 0) // heads
    place = lax.broadcasted_iota(jnp.int32, (rows, half), 1)
    blocks = cache // half

    def attend(step, carry):
        k_copy(step).wait()
        first = step * group
        scores = []
        for s in range(group):
            q_seq = queries[pl.ds(pl.multiple_of((first + s) * heads, heads), heads), :]
            scores.append(
                lax.dot_general(
                    q_seq.astype(BF16), keys[first + s], (((1,), (1,)), ((), ())),
                    preferred_element_type=F32,
                )
            )
        scores = jnp.concatenate(scores, axis=0)
        length = jnp.zeros((rows, 1), jnp.int32)
        for s in range(group):
            length = jnp.where(seq_of == s, lengths_ref[first + s], length)
        opened, pieces, heads_first = [], [], []
        for n in range(blocks):
            z = scores[:, n * half:(n + 1) * half] * HEAD_DIM ** (-0.5) + bias
            shared = jnp.log(1.0 + jnp.exp(-jnp.abs(z)))
            visible = place + n * half < length
            kept = jnp.where(visible, -(jnp.maximum(z, 0.0) + shared), 0.0)
            opened.append(jnp.where(visible, jnp.minimum(z, 0.0) - shared, -jnp.inf))
            coarse = kept.astype(BF16)
            fine = (kept - coarse.astype(F32)).astype(BF16)
            pieces.append(jnp.concatenate([coarse, fine], axis=1))
            heads_first.append(kept[:, 0:1])
        after = jnp.dot(
            jnp.concatenate(pieces, axis=0), later[...], preferred_element_type=F32
        )
        beyond = jnp.zeros((rows, 1), F32)
        weights = [None] * blocks
        for n in reversed(range(blocks)):
            within = after[n * rows:(n + 1) * rows]
            weights[n] = jnp.exp(opened[n] + within + beyond).astype(BF16)
            beyond = beyond + within[:, 0:1] + heads_first[n]
        weights = jnp.concatenate(weights, axis=1)
        v_copy(step).wait()
        for s in range(group):
            mixed[pl.ds(pl.multiple_of((first + s) * heads, heads), heads), :] = jnp.dot(
                weights[s * heads:(s + 1) * heads], values[first + s],
                preferred_element_type=F32,
            )
        return carry

    lax.fori_loop(0, groups, attend, 0)

    copy_wk.wait()
    copy_wv.wait()
    new_keys_ref[...] = jnp.dot(normed, wk[...], preferred_element_type=F32).astype(BF16)
    new_values_ref[...] = jnp.dot(normed, wv[...], preferred_element_type=F32).astype(BF16)

    joined = []
    for pair in range(pairs):
        first = mixed[pl.ds(2 * pair, seqs, stride=heads), :]
        second = mixed[pl.ds(2 * pair + 1, seqs, stride=heads), :]
        if 2 * pair < heads // 2:
            second = pltpu.roll(second, HEAD_DIM, 1)
        else:
            first = pltpu.roll(first, HEAD_DIM, 1)
        joined.append(jnp.where(low, first, second).astype(BF16))
    heads_out = jnp.concatenate(joined, axis=1)
    total = jnp.zeros((seqs, width), F32)
    for i in range(o_parts):
        o_copy(i).wait()
        total += jnp.dot(
            heads_out[:, i * o_rows:(i + 1) * o_rows],
            wo[i * o_rows:(i + 1) * o_rows, :],
            preferred_element_type=F32,
        )
    partial[...] = total
    own = lax.axis_index("tp") * row_count
    other = seqs - row_count - own
    keep_ref[...] = partial[pl.ds(pl.multiple_of(own, 8), row_count), :].astype(BF16)
    send_ref[...] = partial[pl.ds(pl.multiple_of(other, 8), row_count), :].astype(BF16)


def attention(tokens, norm_attn, w_query, w_key, w_value, w_out, attn_bias,
              cache_keys, cache_values, lengths, row_count):
    seqs, width = tokens.shape
    q_width = w_query.shape[1]
    kv_width = w_key.shape[1]
    heads = q_width // HEAD_DIM
    group = 4 if seqs % 4 == 0 else 1
    q_parts = split_of(width, 4)
    o_parts = split_of(q_width, 4)
    dma = pltpu.SemaphoreType.DMA
    half = jax.ShapeDtypeStruct((row_count, width), BF16)
    kv = jax.ShapeDtypeStruct((seqs, kv_width), BF16)
    return pl.pallas_call(
        functools.partial(attention_kernel, row_count, group),
        out_shape=(half, half, kv, kv),
        in_specs=[SMEM, VMEM, VMEM, SMEM] + [ANY] * 6,
        out_specs=(VMEM,) * 4,
        scratch_shapes=[
            pltpu.VMEM(w_query.shape, BF16),
            pltpu.VMEM(w_key.shape, BF16),
            pltpu.VMEM(w_value.shape, BF16),
            pltpu.VMEM(w_out.shape, BF16),
            pltpu.VMEM(cache_keys.shape, BF16),
            pltpu.VMEM(cache_values.shape, BF16),
            pltpu.VMEM((seqs * heads, LANES), F32),
            pltpu.VMEM((seqs * heads, LANES), F32),
            pltpu.VMEM((4 * LANES, 2 * LANES), BF16),
            pltpu.VMEM((seqs, width), F32),
            dma((q_parts,)), dma((2,)), dma((seqs // group,)), dma((seqs // group,)),
            dma((o_parts,)),
        ],
        compiler_params=pltpu.CompilerParams(vmem_limit_bytes=36 * 2**20),
        name="attention",
    )(lengths, tokens, norm_attn.reshape(1, -1), attn_bias,
      w_query, w_key, w_value, w_out, cache_keys, cache_values)


def middle_kernel(row_count, tokens_ref, keep_ref, got_ref, gain_ref, mix_ref, routes_ref,
                  weights_ref, out_ref, middle_ref, wide):
    width = keep_ref.shape[1]
    wide[...] = tokens_ref[...].astype(F32)
    own = pl.multiple_of(lax.axis_index("tp") * row_count, 8)
    attn_sum = keep_ref[...].astype(F32) + got_ref[...].astype(F32)
    middle = (wide[pl.ds(own, row_count), :] + attn_sum).astype(BF16)
    middle_ref[...] = middle
    normed = normed_block(middle.astype(F32), gain_ref[...])
    out_ref[:, :width] = normed
    dot = jnp.sum(normed.astype(F32) * mix_ref[...].astype(F32), axis=-1, keepdims=True)
    gate = 1.0 / (1.0 + jnp.exp(-dot))
    coarse = gate.astype(BF16).astype(F32)
    lane = lax.broadcasted_iota(jnp.int32, (row_count, LANES), 1)
    extra = jnp.where(lane == EXPERTS, coarse, 0.0)
    extra = jnp.where(lane == EXPERTS + 1, gate - coarse, extra)
    for choice in range(routes_ref.shape[1]):
        extra += jnp.where(
            lane == routes_ref[:, choice:choice + 1],
            weights_ref[:, choice:choice + 1].astype(F32), 0.0,
        )
    out_ref[:, width:] = extra.astype(BF16)


def make_middle(tokens, keep, got, norm_ffn, dense_mix, routes, route_weights):
    row_count, width = keep.shape
    return pl.pallas_call(
        functools.partial(middle_kernel, row_count),
        out_shape=(
            jax.ShapeDtypeStruct((row_count, width + LANES), BF16),
            jax.ShapeDtypeStruct((row_count, width), BF16),
        ),
        in_specs=[VMEM] * 7,
        out_specs=(VMEM,) * 2,
        scratch_shapes=[pltpu.VMEM(tokens.shape, F32)],
        compiler_params=pltpu.CompilerParams(vmem_limit_bytes=4 * 2**20),
        name="middle",
    )(tokens, keep, got, norm_ffn.reshape(1, -1), dense_mix.reshape(1, -1), routes,
      route_weights)


def ffn_kernel(
    members, block, out_block,
    rows_ref, eg_hbm, eu_hbm, ed_hbm, dg_hbm, du_hbm, dd_hbm,
    own_ref, other_ref,
    eg, eu, ed, dg, du, dd, eh, dh, sem_e, sem_d, sem_down,
):
    count, padded = rows_ref.shape
    width = padded - LANES
    hidden = eh.shape[0]
    out_blocks = ed.shape[0]

    def gate_copy(i):
        cols = pl.ds(i * block, block)
        return pltpu.make_async_copy(eg_hbm.at[:, cols], eg.at[i], sem_e.at[0, i])

    def up_copy(i):
        cols = pl.ds(i * block, block)
        return pltpu.make_async_copy(eu_hbm.at[:, cols], eu.at[i], sem_e.at[1, i])

    def down_copy(i):
        cols = pl.ds(i * out_block, out_block)
        return pltpu.make_async_copy(ed_hbm.at[:, cols], ed.at[i], sem_down.at[0, i])

    def dense_down_copy(i):
        cols = pl.ds(i * out_block, out_block)
        return pltpu.make_async_copy(dd_hbm.at[:, cols], dd.at[i], sem_down.at[1, i])

    copy_dg = pltpu.make_async_copy(dg_hbm, dg, sem_d.at[0])
    copy_du = pltpu.make_async_copy(du_hbm, du, sem_d.at[1])
    for i in range(hidden):
        gate_copy(i).start()
        up_copy(i).start()
    copy_dg.start()
    copy_du.start()
    for i in range(out_blocks):
        down_copy(i).start()
        dense_down_copy(i).start()

    device = lax.axis_index("ep") * lax.axis_size("tp") + lax.axis_index("tp")
    expert = device // members
    extra = rows_ref[:, width:].astype(F32)
    lane = lax.broadcasted_iota(jnp.int32, extra.shape, 1)
    share = jnp.sum(jnp.where(lane == expert, extra, 0.0), axis=-1, keepdims=True)
    gated = (lane == EXPERTS) | (lane == EXPERTS + 1)
    mix = jnp.sum(jnp.where(gated, extra, 0.0), axis=-1, keepdims=True)
    mix = mix * (1.0 / lax.axis_size("tp"))

    def hidden_of(gate_w, up_w, scale):
        rows = rows_ref[:, :width]
        gate = jnp.dot(rows, gate_w, preferred_element_type=F32)
        up = jnp.dot(rows, up_w, preferred_element_type=F32)
        return (gate / (1.0 + jnp.exp(-gate)) * up * scale).astype(BF16)

    def expert_step(i, carry):
        gate_copy(i).wait()
        up_copy(i).wait()
        eh[i] = hidden_of(eg[i], eu[i], share)
        return carry

    lax.fori_loop(0, hidden, expert_step, 0)
    copy_dg.wait()
    copy_du.wait()
    dh[...] = hidden_of(dg[...], du[...], mix)

    def out_step(i, carry):
        down_copy(i).wait()
        dense_down_copy(i).wait()
        total = jnp.dot(dh[...], dd[i], preferred_element_type=F32)
        for j in range(hidden):
            total += jnp.dot(
                eh[j], ed[i, j * block:(j + 1) * block, :], preferred_element_type=F32
            )
        cols = pl.ds(pl.multiple_of(i * out_block, out_block), out_block)
        own_ref[:, cols] = total[:count // 2]
        other_ref[:, cols] = total[count // 2:].astype(BF16)
        return carry

    lax.fori_loop(0, out_blocks, out_step, 0)


def feed_forward(rows, expert_gate, expert_up, expert_down, dense_gate_w, dense_up_w,
                 dense_down_w, members):
    count, padded = rows.shape
    width = padded - LANES
    units = expert_gate.shape[1]
    block = 256 if units % 256 == 0 else units
    hidden = units // block
    out_block = 256 if width % 256 == 0 else width
    out_blocks = width // out_block
    dense_units = dense_gate_w.shape[1]
    dma = pltpu.SemaphoreType.DMA
    return pl.pallas_call(
        functools.partial(ffn_kernel, members, block, out_block),
        out_shape=(
            jax.ShapeDtypeStruct((count // 2, width), F32),
            jax.ShapeDtypeStruct((count // 2, width), BF16),
        ),
        in_specs=[VMEM] + [ANY] * 6,
        out_specs=(VMEM,) * 2,
        scratch_shapes=[
            pltpu.VMEM((hidden, width, block), BF16),
            pltpu.VMEM((hidden, width, block), BF16),
            pltpu.VMEM((out_blocks, units, out_block), BF16),
            pltpu.VMEM(dense_gate_w.shape, BF16),
            pltpu.VMEM(dense_up_w.shape, BF16),
            pltpu.VMEM((out_blocks, dense_units, out_block), BF16),
            pltpu.VMEM((hidden, count, block), BF16),
            pltpu.VMEM((count, dense_units), BF16),
            dma((2, hidden)), dma((2,)), dma((2, out_blocks)),
        ],
        compiler_params=pltpu.CompilerParams(vmem_limit_bytes=46 * 2**20),
        name="feed_forward",
    )(rows, expert_gate, expert_up, expert_down, dense_gate_w, dense_up_w, dense_down_w)


def phases_of(n_ep):
    bits = [1 << b for b in range(n_ep.bit_length() - 1)]
    phases = []
    while len(bits) >= 2:
        high, low = bits.pop(), bits.pop()
        phases += [(low, high), (high, low)]
    return phases + [(bit, bit) for bit in bits]


def exchange(array, masks, n_ep, n_tp):
    pairs = [
        (ep * n_tp + tp, (ep ^ masks[tp % 2]) * n_tp + tp)
        for ep in range(n_ep) for tp in range(n_tp)
    ]
    return lax.ppermute(array, ("ep", "tp"), pairs)


def swap(array, n_tp):
    return lax.ppermute(array, "tp", [(i, i ^ 1) for i in range(n_tp)])


def shards(
    tokens, norm_attn, w_query, w_key, w_value, w_out, attn_bias, cache_keys, cache_values,
    lengths, norm_ffn, expert_gate, expert_up, expert_down, dense_gate_w, dense_up_w,
    dense_down_w, dense_mix, routes, route_weights,
):
    n_ep, n_tp = lax.axis_size("ep"), lax.axis_size("tp")
    row_count = tokens.shape[0] // n_tp
    keep, send, new_keys, new_values = attention(
        tokens, norm_attn, w_query, w_key, w_value, w_out, attn_bias, cache_keys,
        cache_values, lengths, row_count,
    )
    rows, middle = make_middle(
        tokens, keep, swap(send, n_tp), norm_ffn, dense_mix, routes, route_weights
    )
    phases = phases_of(n_ep)
    for masks in phases:
        rows = jnp.concatenate([rows, exchange(rows, masks, n_ep, n_tp)], axis=0)
    rows = jnp.concatenate([rows, swap(rows, n_tp)], axis=0)
    own, other = feed_forward(
        rows, expert_gate, expert_up, expert_down, dense_gate_w, dense_up_w, dense_down_w,
        n_ep * n_tp // EXPERTS,
    )
    total = own + swap(other, n_tp).astype(F32)
    for masks in reversed(phases):
        half = total.shape[0] // 2
        got = exchange(total[half:].astype(BF16), masks, n_ep, n_tp)
        total = total[:half] + got.astype(F32)
    layer_out = (middle.astype(F32) + total).astype(BF16)
    return layer_out, new_keys, new_values


def solution(mesh):
    placed = (
        P("ep", None),
        P(),
        P(None, "tp"),
        P(None, "tp"),
        P(None, "tp"),
        P("tp", None),
        P("tp"),
        P("ep", None, "tp"),
        P("ep", None, "tp"),
        P("ep"),
        P(),
        P(None, ("ep", "tp")),
        P(None, ("ep", "tp")),
        P(("ep", "tp"), None),
        P(None, "ep"),
        P(None, "ep"),
        P("ep", None),
        P(),
        P(("ep", "tp"), None),
        P(("ep", "tp"), None),
    )
    return jax.shard_map(
        shards,
        mesh=mesh,
        in_specs=placed,
        out_specs=(P(("ep", "tp"), None), P("ep", "tp"), P("ep", "tp")),
        check_vma=False,
    )
```

```python
import functools
import math

import jax
import jax.numpy as jnp
from jax import lax
from jax.experimental import pallas as pl
from jax.experimental.pallas import tpu as pltpu
from jax.sharding import PartitionSpec as P

HEAD_DIM = 64
EXPERTS = 8
LANES = 128
EPSILON = 1e-06
FETCH_FLOPS = 200
F32 = jnp.float32
BF16 = jnp.bfloat16


HBM = pl.BlockSpec(memory_space=pltpu.HBM)
VMEM = pl.BlockSpec(memory_space=pltpu.VMEM)


def in_hbm(*arrays):
    return [pltpu.with_memory_space_constraint(array, pltpu.HBM) for array in arrays]


def split_of(total, most):
    for pieces in range(most, 0, -1):
        if total % (pieces * 256) == 0:
            return pieces
    return 1


def normed_block(widened, gain):
    scale = lax.rsqrt(jnp.mean(widened * widened, axis=-1, keepdims=True) + EPSILON)
    return (widened * scale * gain).astype(BF16)


def attention_kernel(
    row_count, group,
    lengths_hbm, tokens_hbm, gain_hbm, bias_hbm,
    wq_hbm, wk_hbm, wv_hbm, wo_hbm, keys_hbm, values_hbm,
    keep_ref, send_ref, new_keys_ref, new_values_ref,
    lengths_ref, tokens_ref, gain_ref, bias_ref,
    wq, wk, wv, wo, keys, values, queries, mixed, later, partial,
    sem_small, sem_q, sem_kv, sem_k, sem_v, sem_o,
):
    seqs, width = tokens_ref.shape
    cache = keys.shape[1]
    q_width = wq.shape[1]
    heads = q_width // HEAD_DIM
    pairs = heads // 2
    q_parts = sem_q.shape[0]
    o_parts = sem_o.shape[0]
    groups = seqs // group
    q_rows = width // q_parts
    o_rows = q_width // o_parts
    half = 2 * LANES

    def q_copy(i):
        rows = pl.ds(i * q_rows, q_rows)
        return pltpu.make_async_copy(wq_hbm.at[rows], wq.at[rows], sem_q.at[i])

    def o_copy(i):
        rows = pl.ds(i * o_rows, o_rows)
        return pltpu.make_async_copy(wo_hbm.at[rows], wo.at[rows], sem_o.at[i])

    def k_copy(i):
        rows = pl.ds(i * group, group)
        return pltpu.make_async_copy(keys_hbm.at[rows], keys.at[rows], sem_k.at[i])

    def v_copy(i):
        rows = pl.ds(i * group, group)
        return pltpu.make_async_copy(values_hbm.at[rows], values.at[rows], sem_v.at[i])

    small = [
        pltpu.make_async_copy(source, target, sem_small.at[i])
        for i, (source, target) in enumerate((
            (tokens_hbm, tokens_ref), (gain_hbm, gain_ref),
            (lengths_hbm, lengths_ref), (bias_hbm, bias_ref),
        ))
    ]
    for copy in small:
        copy.start()
    copy_wk = pltpu.make_async_copy(wk_hbm, wk, sem_kv.at[0])
    copy_wv = pltpu.make_async_copy(wv_hbm, wv, sem_kv.at[1])
    for i in range(q_parts):
        q_copy(i).start()
    for i in range(groups):
        k_copy(i).start()
        v_copy(i).start()
    copy_wk.start()
    copy_wv.start()
    for i in range(o_parts):
        o_copy(i).start()

    later_rows = lax.broadcasted_iota(jnp.int32, (2 * half, half), 0) % half
    later_cols = lax.broadcasted_iota(jnp.int32, (2 * half, half), 1)
    later[...] = (later_rows > later_cols).astype(F32).astype(BF16)

    for copy in small:
        copy.wait()
    normed = normed_block(tokens_ref[...].astype(F32), gain_ref[...])
    query = jnp.zeros((seqs, q_width), F32)
    for i in range(q_parts):
        q_copy(i).wait()
        query += jnp.dot(
            normed[:, i * q_rows:(i + 1) * q_rows],
            wq[i * q_rows:(i + 1) * q_rows, :],
            preferred_element_type=F32,
        )
    query = query.astype(BF16).astype(F32)

    lane = lax.broadcasted_iota(jnp.int32, (seqs, LANES), 1)
    low = lane < HEAD_DIM
    for pair in range(pairs):
        both = query[:, pair * LANES:(pair + 1) * LANES]
        turned = pltpu.roll(both, HEAD_DIM, 1)
        if 2 * pair < heads // 2:
            first, second = jnp.where(low, both, 0.0), jnp.where(low, turned, 0.0)
        else:
            first, second = jnp.where(low, 0.0, turned), jnp.where(low, 0.0, both)
        queries[pl.ds(2 * pair, seqs, stride=heads), :] = first
        queries[pl.ds(2 * pair + 1, seqs, stride=heads), :] = second

    rows = group * heads
    head_of = lax.broadcasted_iota(jnp.int32, (heads, 1), 0)
    bias = jnp.zeros((heads, 1), F32)
    for head in range(heads):
        bias = jnp.where(head_of == head, bias_ref[head], bias)
    bias = jnp.concatenate([bias] * group, axis=0)
    seq_of = lax.broadcasted_iota(jnp.int32, (rows, 1), 0) // heads
    place = lax.broadcasted_iota(jnp.int32, (rows, half), 1)
    blocks = cache // half

    def attend(step, carry):
        k_copy(step).wait()
        first = step * group
        scores = []
        for s in range(group):
            q_seq = queries[pl.ds(pl.multiple_of((first + s) * heads, heads), heads), :]
            scores.append(
                lax.dot_general(
                    q_seq.astype(BF16), keys[first + s], (((1,), (1,)), ((), ())),
                    preferred_element_type=F32,
                )
            )
        scores = jnp.concatenate(scores, axis=0)
        length = jnp.zeros((rows, 1), jnp.int32)
        for s in range(group):
            length = jnp.where(seq_of == s, lengths_ref[first + s], length)
        opened, pieces, heads_first = [], [], []
        for n in range(blocks):
            z = scores[:, n * half:(n + 1) * half] * HEAD_DIM ** (-0.5) + bias
            shared = jnp.log(1.0 + jnp.exp(-jnp.abs(z)))
            visible = place + n * half < length
            kept = jnp.where(visible, -(jnp.maximum(z, 0.0) + shared), 0.0)
            opened.append(jnp.where(visible, jnp.minimum(z, 0.0) - shared, -jnp.inf))
            coarse = kept.astype(BF16)
            fine = (kept - coarse.astype(F32)).astype(BF16)
            pieces.append(jnp.concatenate([coarse, fine], axis=1))
            heads_first.append(kept[:, 0:1])
        after = jnp.dot(
            jnp.concatenate(pieces, axis=0), later[...], preferred_element_type=F32
        )
        beyond = jnp.zeros((rows, 1), F32)
        weights = [None] * blocks
        for n in reversed(range(blocks)):
            within = after[n * rows:(n + 1) * rows]
            weights[n] = jnp.exp(opened[n] + within + beyond).astype(BF16)
            beyond = beyond + within[:, 0:1] + heads_first[n]
        weights = jnp.concatenate(weights, axis=1)
        v_copy(step).wait()
        for s in range(group):
            mixed[pl.ds(pl.multiple_of((first + s) * heads, heads), heads), :] = jnp.dot(
                weights[s * heads:(s + 1) * heads], values[first + s],
                preferred_element_type=F32,
            )
        return carry

    lax.fori_loop(0, groups, attend, 0)

    copy_wk.wait()
    copy_wv.wait()
    new_keys_ref[...] = jnp.dot(normed, wk[...], preferred_element_type=F32).astype(BF16)
    new_values_ref[...] = jnp.dot(normed, wv[...], preferred_element_type=F32).astype(BF16)

    joined = []
    for pair in range(pairs):
        first = mixed[pl.ds(2 * pair, seqs, stride=heads), :]
        second = mixed[pl.ds(2 * pair + 1, seqs, stride=heads), :]
        if 2 * pair < heads // 2:
            second = pltpu.roll(second, HEAD_DIM, 1)
        else:
            first = pltpu.roll(first, HEAD_DIM, 1)
        joined.append(jnp.where(low, first, second).astype(BF16))
    heads_out = jnp.concatenate(joined, axis=1)
    total = jnp.zeros((seqs, width), F32)
    for i in range(o_parts):
        o_copy(i).wait()
        total += jnp.dot(
            heads_out[:, i * o_rows:(i + 1) * o_rows],
            wo[i * o_rows:(i + 1) * o_rows, :],
            preferred_element_type=F32,
        )
    partial[...] = total
    own = lax.axis_index("tp") * row_count
    other = seqs - row_count - own
    keep_ref[...] = partial[pl.ds(pl.multiple_of(own, 8), row_count), :].astype(BF16)
    send_ref[...] = partial[pl.ds(pl.multiple_of(other, 8), row_count), :].astype(BF16)


def attention(tokens, norm_attn, w_query, w_key, w_value, w_out, attn_bias,
              cache_keys, cache_values, lengths, row_count):
    seqs, width = tokens.shape
    q_width = w_query.shape[1]
    kv_width = w_key.shape[1]
    heads = q_width // HEAD_DIM
    group = 4 if seqs % 4 == 0 else 1
    q_parts = split_of(width, 4)
    o_parts = split_of(q_width, 4)
    dma = pltpu.SemaphoreType.DMA
    half = jax.ShapeDtypeStruct((row_count, width), BF16)
    kv = jax.ShapeDtypeStruct((seqs, kv_width), BF16)
    return pl.pallas_call(
        functools.partial(attention_kernel, row_count, group),
        out_shape=(half, half, kv, kv),
        in_specs=[HBM] * 10,
        out_specs=(VMEM,) * 4,
        scratch_shapes=[
            pltpu.SMEM(lengths.shape, jnp.int32),
            pltpu.VMEM(tokens.shape, BF16),
            pltpu.VMEM((1, width), F32),
            pltpu.SMEM(attn_bias.shape, F32),
            pltpu.VMEM(w_query.shape, BF16),
            pltpu.VMEM(w_key.shape, BF16),
            pltpu.VMEM(w_value.shape, BF16),
            pltpu.VMEM(w_out.shape, BF16),
            pltpu.VMEM(cache_keys.shape, BF16),
            pltpu.VMEM(cache_values.shape, BF16),
            pltpu.VMEM((seqs * heads, LANES), F32),
            pltpu.VMEM((seqs * heads, LANES), F32),
            pltpu.VMEM((4 * LANES, 2 * LANES), BF16),
            pltpu.VMEM((seqs, width), F32),
            dma((4,)), dma((q_parts,)), dma((2,)), dma((seqs // group,)), dma((seqs // group,)),
            dma((o_parts,)),
        ],
        compiler_params=pltpu.CompilerParams(vmem_limit_bytes=36 * 2**20),
        name="attention",
    )(*in_hbm(lengths, tokens, norm_attn.reshape(1, -1), attn_bias, w_query, w_key,
              w_value, w_out, cache_keys, cache_values))


def middle_kernel(row_count, tokens_ref, keep_ref, got_ref, gain_ref, mix_ref, routes_ref,
                  weights_ref, out_ref, middle_ref, wide):
    width = keep_ref.shape[1]
    wide[...] = tokens_ref[...].astype(F32)
    own = pl.multiple_of(lax.axis_index("tp") * row_count, 8)
    attn_sum = keep_ref[...].astype(F32) + got_ref[...].astype(F32)
    middle = (wide[pl.ds(own, row_count), :] + attn_sum).astype(BF16)
    middle_ref[...] = middle
    normed = normed_block(middle.astype(F32), gain_ref[...])
    out_ref[:, :width] = normed
    dot = jnp.sum(normed.astype(F32) * mix_ref[...].astype(F32), axis=-1, keepdims=True)
    gate = 1.0 / (1.0 + jnp.exp(-dot))
    coarse = gate.astype(BF16).astype(F32)
    lane = lax.broadcasted_iota(jnp.int32, (row_count, LANES), 1)
    extra = jnp.where(lane == EXPERTS, coarse, 0.0)
    extra = jnp.where(lane == EXPERTS + 1, gate - coarse, extra)
    for choice in range(routes_ref.shape[1]):
        extra += jnp.where(
            lane == routes_ref[:, choice:choice + 1],
            weights_ref[:, choice:choice + 1].astype(F32), 0.0,
        )
    out_ref[:, width:] = extra.astype(BF16)


def make_middle(tokens, keep, got, norm_ffn, dense_mix, routes, route_weights):
    row_count, width = keep.shape
    return pl.pallas_call(
        functools.partial(middle_kernel, row_count),
        out_shape=(
            jax.ShapeDtypeStruct((row_count, width + LANES), BF16),
            jax.ShapeDtypeStruct((row_count, width), BF16),
        ),
        in_specs=[VMEM] * 7,
        out_specs=(VMEM,) * 2,
        scratch_shapes=[pltpu.VMEM(tokens.shape, F32)],
        compiler_params=pltpu.CompilerParams(vmem_limit_bytes=4 * 2**20),
        name="middle",
    )(tokens, keep, got, norm_ffn.reshape(1, -1), dense_mix.reshape(1, -1), routes,
      route_weights)


def units_part(units):
    return pl.ds(pl.multiple_of(lax.axis_index("tp") * units, 8), units)


def fetch_all(copies, sems):
    copies = [
        pltpu.make_async_copy(source, target, sems.at[i])
        for i, (source, target) in enumerate(copies)
    ]
    for copy in copies:
        copy.start()
    for copy in copies:
        copy.wait()


def fetch_up_kernel(after_hbm, gate_hbm, up_hbm, dense_gate_hbm, dense_up_hbm, wide, dense, sems):
    hidden, _, block = wide.shape
    part = units_part(dense.shape[1])
    copies = []
    if block == gate_hbm.shape[1]:
        copies += [(gate_hbm, wide.at[0]), (up_hbm, wide.at[1])]
    else:
        block //= 2
        for i in range(hidden):
            cols = pl.ds(i * block, block)
            copies.append((gate_hbm.at[:, cols], wide.at[i, :, pl.ds(0, block)]))
            copies.append((up_hbm.at[:, cols], wide.at[i, :, pl.ds(block, block)]))
    copies.append((dense_gate_hbm.at[part], dense.at[0]))
    copies.append((dense_up_hbm.at[part], dense.at[1]))
    fetch_all(copies, sems)


def fetch_down_kernel(after_hbm, down_hbm, dense_down_hbm, down, dense, sems):
    pieces = sems.shape[0] // 2
    rows = down.shape[0] // pieces
    dense_rows = dense.shape[0] // pieces
    first = units_part(dense.shape[0]).start
    copies = []
    for i in range(pieces):
        part = pl.ds(i * rows, rows)
        copies.append((down_hbm.at[part], down.at[part]))
        source = pl.ds(pl.multiple_of(first + i * dense_rows, 8), dense_rows)
        copies.append((dense_down_hbm.at[source], dense.at[pl.ds(i * dense_rows, dense_rows)]))
    fetch_all(copies, sems)


def fetch_call(kernel, after, arrays, shapes, copies):
    size = sum(2 * math.prod(shape) for shape in shapes)
    return pl.pallas_call(
        kernel,
        out_shape=tuple(pltpu.VMEM(shape, BF16) for shape in shapes),
        in_specs=[HBM] * (1 + len(arrays)),
        out_specs=(VMEM,) * len(shapes),
        scratch_shapes=[pltpu.SemaphoreType.DMA((copies,))],
        cost_estimate=pl.CostEstimate(
            flops=FETCH_FLOPS * size, bytes_accessed=size, transcendentals=0
        ),
        compiler_params=pltpu.CompilerParams(vmem_limit_bytes=2**20),
    )(after, *in_hbm(*arrays))


def fetch_weights(after_first, after_second, expert_gate, expert_up, expert_down, dense_gate_w,
                  dense_up_w, dense_down_w):
    width, units = expert_gate.shape
    wide = (units // 256, width, 512) if units % 512 == 256 else (2, width, units)
    dense_units = dense_gate_w.shape[1] // lax.axis_size("tp")
    pieces = 4 if units % 64 == 0 and dense_units % 32 == 0 else 1
    down, dense_down = fetch_call(
        fetch_down_kernel, after_first, (expert_down, dense_down_w),
        ((units, width), (dense_units, width)), 2 * pieces,
    )
    wide, dense = fetch_call(
        fetch_up_kernel, after_second,
        (expert_gate, expert_up, dense_gate_w.T, dense_up_w.T),
        (wide, (2, dense_units, width)), 2 * max(wide[0], 1) + 2,
    )
    return wide, dense, down, dense_down


def ffn_kernel(members, out_block, rows_ref, wide, dense, down, dense_down, own_ref, other_ref,
               hidden_ref):
    count, padded = rows_ref.shape
    width = padded - LANES
    units = down.shape[0]
    hidden, _, block = wide.shape
    device = lax.axis_index("ep") * lax.axis_size("tp") + lax.axis_index("tp")
    expert = device // members
    extra = rows_ref[:, width:].astype(F32)
    lane = lax.broadcasted_iota(jnp.int32, extra.shape, 1)
    share = jnp.sum(jnp.where(lane == expert, extra, 0.0), axis=-1, keepdims=True)
    gated = (lane == EXPERTS) | (lane == EXPERTS + 1)
    mix = jnp.sum(jnp.where(gated, extra, 0.0), axis=-1, keepdims=True)

    def activate(gate, up, scale):
        return (gate / (1.0 + jnp.exp(-gate)) * up * scale).astype(BF16)

    rows = rows_ref[:, :width]
    if block == units:
        gate, up = (jnp.dot(rows, wide[i], preferred_element_type=F32) for i in range(2))
        hidden_ref[...] = activate(gate, up, share)
    else:
        block //= 2
        for i in range(hidden):
            both = jnp.dot(rows, wide[i], preferred_element_type=F32)
            hidden_ref[:, i * block:(i + 1) * block] = activate(
                both[:, :block], both[:, block:], share
            )
    dims = (((1,), (1,)), ((), ()))
    gate, up = (
        lax.dot_general(rows, dense[i], dims, preferred_element_type=F32) for i in range(2)
    )
    dense_hidden = activate(gate, up, mix)
    for first in range(0, width, out_block):
        cols = slice(first, first + out_block)
        total = jnp.dot(hidden_ref[...], down[:, cols], preferred_element_type=F32)
        total += jnp.dot(dense_hidden, dense_down[:, cols], preferred_element_type=F32)
        own_ref[:, cols] = total[:count // 2]
        other_ref[:, cols] = total[count // 2:].astype(BF16)


def feed_forward(rows, weights, members):
    count, padded = rows.shape
    width = padded - LANES
    units = weights[2].shape[0]
    return pl.pallas_call(
        functools.partial(ffn_kernel, members, 512 if width % 512 == 0 else width),
        out_shape=(
            jax.ShapeDtypeStruct((count // 2, width), F32),
            jax.ShapeDtypeStruct((count // 2, width), BF16),
        ),
        in_specs=[VMEM] * 5,
        out_specs=(VMEM,) * 2,
        scratch_shapes=[pltpu.VMEM((count, units), BF16)],
        cost_estimate=pl.CostEstimate(
            flops=6 * count * width * units, bytes_accessed=0, transcendentals=0
        ),
        compiler_params=pltpu.CompilerParams(vmem_limit_bytes=16 * 2**20),
        name="feed_forward",
    )(rows, *weights)


def phases_of(n_ep):
    bits = [1 << b for b in range(n_ep.bit_length() - 1)]
    phases = []
    while len(bits) >= 2:
        high, low = bits.pop(), bits.pop()
        phases += [(low, high), (high, low)]
    return phases + [(bit, bit) for bit in bits]


def exchange(array, masks, n_ep, n_tp):
    pairs = [
        (ep * n_tp + tp, (ep ^ masks[tp % 2]) * n_tp + tp)
        for ep in range(n_ep) for tp in range(n_tp)
    ]
    return lax.ppermute(array, ("ep", "tp"), pairs)


def swap(array, n_tp):
    return lax.ppermute(array, "tp", [(i, i ^ 1) for i in range(n_tp)])


def layer(
    tokens, norm_attn, w_query, w_key, w_value, w_out, attn_bias, cache_keys, cache_values,
    lengths, norm_ffn, expert_gate, expert_up, expert_down, dense_gate_w, dense_up_w,
    dense_down_w, dense_mix, routes, route_weights,
):
    n_ep, n_tp = lax.axis_size("ep"), lax.axis_size("tp")
    row_count = tokens.shape[0] // n_tp
    keep, send, new_keys, new_values = attention(
        tokens, norm_attn, w_query, w_key, w_value, w_out, attn_bias, cache_keys,
        cache_values, lengths, row_count,
    )
    rows, middle = make_middle(
        tokens, keep, swap(send, n_tp), norm_ffn, dense_mix, routes, route_weights
    )
    phases = phases_of(n_ep)
    held = []
    for masks in phases:
        held.append(rows)
        got = exchange(rows, masks, n_ep, n_tp)
        rows = jnp.concatenate([rows, got], axis=0)
    weights = fetch_weights(
        held[-2], held[-1], expert_gate, expert_up, expert_down, dense_gate_w, dense_up_w,
        dense_down_w,
    )
    rows = jnp.concatenate([rows, swap(rows, n_tp)], axis=0)
    own, other = feed_forward(rows, weights, n_ep * n_tp // EXPERTS)
    total = own + swap(other, n_tp).astype(F32)
    for masks in reversed(phases):
        half = total.shape[0] // 2
        got = exchange(total[half:].astype(BF16), masks, n_ep, n_tp)
        total = total[:half] + got.astype(F32)
    layer_out = (middle.astype(F32) + total).astype(BF16)
    return layer_out, new_keys, new_values


def solution(mesh):
    placed = (
        P("ep", None),
        P(),
        P(None, "tp"),
        P(None, "tp"),
        P(None, "tp"),
        P("tp", None),
        P("tp"),
        P("ep", None, "tp"),
        P("ep", None, "tp"),
        P("ep"),
        P(),
        P(None, ("ep", "tp")),
        P(None, ("ep", "tp")),
        P(("ep", "tp"), None),
        P(None, "ep"),
        P(None, "ep"),
        P("ep", None),
        P(),
        P(("ep", "tp"), None),
        P(("ep", "tp"), None),
    )
    return jax.shard_map(
        layer,
        mesh=mesh,
        in_specs=placed,
        out_specs=(P(("ep", "tp"), None), P("ep", "tp"), P("ep", "tp")),
        check_vma=False,
    )
```

```python
import functools
import math

import jax
import jax.numpy as jnp
from jax import lax
from jax.experimental import pallas as pl
from jax.experimental.pallas import tpu as pltpu
from jax.sharding import PartitionSpec as P

HEAD_DIM = 64
EXPERTS = 8
LANES = 128
BLOCK = 256
EPSILON = 1e-06
FETCH_FLOPS = 200
IN_FLIGHT = 8
GROUP = 8
F32 = jnp.float32
BF16 = jnp.bfloat16


HBM = pl.BlockSpec(memory_space=pltpu.HBM)
VMEM = pl.BlockSpec(memory_space=pltpu.VMEM)


def in_hbm(*arrays):
    return [pltpu.with_memory_space_constraint(array, pltpu.HBM) for array in arrays]


def split_of(total, most):
    for pieces in range(most, 0, -1):
        if total % (pieces * 256) == 0:
            return pieces
    return 1


def normed_block(widened, gain):
    scale = lax.rsqrt(jnp.mean(widened * widened, axis=-1, keepdims=True) + EPSILON)
    return (widened * scale * gain).astype(BF16)


def attention_kernel(
    row_count, group, q_parts, o_parts,
    lengths_hbm, tokens_hbm, gain_hbm, bias_hbm,
    wq_hbm, wk_hbm, wv_hbm, wo_hbm, keys_hbm, values_hbm,
    keep_ref, send_ref, new_keys_ref, new_values_ref,
    lengths_ref, tokens_ref, gain_ref, bias_ref,
    wq, wk, wv, wo, keys, values, queries, mixed, later, partial,
    sems,
):
    seqs, width = tokens_ref.shape
    cache = keys.shape[1]
    q_width = wq.shape[1]
    heads = q_width // HEAD_DIM
    pairs = heads // 2
    groups = seqs // group
    q_rows = width // q_parts
    o_rows = q_width // o_parts
    half = 2 * LANES

    plan = [
        (tokens_hbm, tokens_ref), (gain_hbm, gain_ref), (lengths_hbm, lengths_ref),
        (bias_hbm, bias_ref),
    ]
    small = len(plan)
    for i in range(q_parts):
        part = pl.ds(i * q_rows, q_rows)
        plan.append((wq_hbm.at[part], wq.at[part]))
    parts = [pl.ds(i * group, group) for i in range(groups)]
    plan.append((keys_hbm.at[parts[0]], keys.at[parts[0]]))
    for i in range(groups):
        for part in parts[i + 1:i + 2]:
            plan.append((keys_hbm.at[part], keys.at[part]))
        plan.append((values_hbm.at[parts[i]], values.at[parts[i]]))
    plan += [(wk_hbm, wk), (wv_hbm, wv)]
    for i in range(o_parts):
        part = pl.ds(i * o_rows, o_rows)
        plan.append((wo_hbm.at[part], wo.at[part]))
    copies = [
        pltpu.make_async_copy(source, target, sems.at[i])
        for i, (source, target) in enumerate(plan)
    ]
    waited = [0]
    for copy in copies[:small + IN_FLIGHT]:
        copy.start()

    def arrive(count):
        for _ in range(count):
            copies[waited[0]].wait()
            waited[0] += 1
            following = waited[0] + IN_FLIGHT - 1
            if waited[0] > small and following < len(copies):
                copies[following].start()

    later_rows = lax.broadcasted_iota(jnp.int32, (2 * half, half), 0) % half
    later_cols = lax.broadcasted_iota(jnp.int32, (2 * half, half), 1)
    later[...] = (later_rows > later_cols).astype(F32).astype(BF16)

    arrive(small)
    normed = normed_block(tokens_ref[...].astype(F32), gain_ref[...])
    query = jnp.zeros((seqs, q_width), F32)
    for i in range(q_parts):
        arrive(1)
        query += jnp.dot(
            normed[:, i * q_rows:(i + 1) * q_rows],
            wq[i * q_rows:(i + 1) * q_rows, :],
            preferred_element_type=F32,
        )
    query = query.astype(BF16).astype(F32)

    lane = lax.broadcasted_iota(jnp.int32, (seqs, LANES), 1)
    low = lane < HEAD_DIM
    for pair in range(pairs):
        both = query[:, pair * LANES:(pair + 1) * LANES]
        turned = pltpu.roll(both, HEAD_DIM, 1)
        if 2 * pair < heads // 2:
            first, second = jnp.where(low, both, 0.0), jnp.where(low, turned, 0.0)
        else:
            first, second = jnp.where(low, 0.0, turned), jnp.where(low, 0.0, both)
        queries[pl.ds(2 * pair, seqs, stride=heads), :] = first
        queries[pl.ds(2 * pair + 1, seqs, stride=heads), :] = second

    rows = group * heads
    head_of = lax.broadcasted_iota(jnp.int32, (heads, 1), 0)
    bias = jnp.zeros((heads, 1), F32)
    for head in range(heads):
        bias = jnp.where(head_of == head, bias_ref[head], bias)
    bias = jnp.concatenate([bias] * group, axis=0)
    seq_of = lax.broadcasted_iota(jnp.int32, (rows, 1), 0) // heads
    place = lax.broadcasted_iota(jnp.int32, (rows, half), 1)
    blocks = cache // half

    def score(step):
        arrive(1)
        scores = []
        for s in range(step * group, (step + 1) * group):
            q_seq = queries[pl.ds(s * heads, heads), :].astype(BF16)
            scores.append(
                lax.dot_general(
                    q_seq, keys[s], (((1,), (1,)), ((), ())), preferred_element_type=F32
                )
            )
        return jnp.concatenate(scores, axis=0)

    def weigh(step, scores):
        length = jnp.zeros((rows, 1), jnp.int32)
        for s in range(group):
            length = jnp.where(seq_of == s, lengths_ref[step * group + s], length)
        opened, pieces, heads_first = [], [], []
        for n in range(blocks):
            z = scores[:, n * half:(n + 1) * half] * HEAD_DIM ** (-0.5) + bias
            shared = jnp.log(1.0 + jnp.exp(-jnp.abs(z)))
            visible = place + n * half < length
            kept = jnp.where(visible, -(jnp.maximum(z, 0.0) + shared), 0.0)
            opened.append(jnp.where(visible, jnp.minimum(z, 0.0) - shared, -jnp.inf))
            coarse = kept.astype(BF16)
            fine = (kept - coarse.astype(F32)).astype(BF16)
            pieces.append(jnp.concatenate([coarse, fine], axis=1))
            heads_first.append(kept[:, 0:1])
        after = jnp.dot(
            jnp.concatenate(pieces, axis=0), later[...], preferred_element_type=F32
        )
        beyond = jnp.zeros((rows, 1), F32)
        weights = [None] * blocks
        for n in reversed(range(blocks)):
            within = after[n * rows:(n + 1) * rows]
            weights[n] = jnp.exp(opened[n] + within + beyond).astype(BF16)
            beyond = beyond + within[:, 0:1] + heads_first[n]
        return jnp.concatenate(weights, axis=1)

    def mix(step, weights):
        arrive(1)
        for s in range(group):
            seq = step * group + s
            mixed[pl.ds(seq * heads, heads), :] = jnp.dot(
                weights[s * heads:(s + 1) * heads], values[seq], preferred_element_type=F32
            )

    scores = score(0)
    for step in range(groups):
        following = score(step + 1) if step + 1 < groups else None
        weights = weigh(step, scores)
        mix(step, weights)
        scores = following

    arrive(2)
    new_keys_ref[...] = jnp.dot(normed, wk[...], preferred_element_type=F32).astype(BF16)
    new_values_ref[...] = jnp.dot(normed, wv[...], preferred_element_type=F32).astype(BF16)

    joined = []
    for pair in range(pairs):
        first = mixed[pl.ds(2 * pair, seqs, stride=heads), :]
        second = mixed[pl.ds(2 * pair + 1, seqs, stride=heads), :]
        if 2 * pair < heads // 2:
            second = pltpu.roll(second, HEAD_DIM, 1)
        else:
            first = pltpu.roll(first, HEAD_DIM, 1)
        joined.append(jnp.where(low, first, second).astype(BF16))
    heads_out = jnp.concatenate(joined, axis=1)
    total = jnp.zeros((seqs, width), F32)
    for i in range(o_parts):
        arrive(1)
        total += jnp.dot(
            heads_out[:, i * o_rows:(i + 1) * o_rows],
            wo[i * o_rows:(i + 1) * o_rows, :],
            preferred_element_type=F32,
        )
    partial[...] = total
    own = lax.axis_index("tp") * row_count
    other = seqs - row_count - own
    keep_ref[...] = partial[pl.ds(pl.multiple_of(own, 8), row_count), :].astype(BF16)
    send_ref[...] = partial[pl.ds(pl.multiple_of(other, 8), row_count), :].astype(BF16)


def attention(tokens, norm_attn, w_query, w_key, w_value, w_out, attn_bias,
              cache_keys, cache_values, lengths, row_count):
    seqs, width = tokens.shape
    q_width = w_query.shape[1]
    kv_width = w_key.shape[1]
    heads = q_width // HEAD_DIM
    group = GROUP if seqs % GROUP == 0 else 1
    q_parts = split_of(width, 4)
    o_parts = split_of(q_width, 4)
    dma = pltpu.SemaphoreType.DMA
    half = jax.ShapeDtypeStruct((row_count, width), BF16)
    kv = jax.ShapeDtypeStruct((seqs, kv_width), BF16)
    return pl.pallas_call(
        functools.partial(attention_kernel, row_count, group, q_parts, o_parts),
        out_shape=(half, half, kv, kv),
        in_specs=[HBM] * 10,
        out_specs=(VMEM,) * 4,
        scratch_shapes=[
            pltpu.SMEM(lengths.shape, jnp.int32),
            pltpu.VMEM(tokens.shape, BF16),
            pltpu.VMEM((1, width), F32),
            pltpu.SMEM(attn_bias.shape, F32),
            pltpu.VMEM(w_query.shape, BF16),
            pltpu.VMEM(w_key.shape, BF16),
            pltpu.VMEM(w_value.shape, BF16),
            pltpu.VMEM(w_out.shape, BF16),
            pltpu.VMEM(cache_keys.shape, BF16),
            pltpu.VMEM(cache_values.shape, BF16),
            pltpu.VMEM((seqs * heads, LANES), F32),
            pltpu.VMEM((seqs * heads, LANES), F32),
            pltpu.VMEM((4 * LANES, 2 * LANES), BF16),
            pltpu.VMEM((seqs, width), F32),
            dma((6 + q_parts + o_parts + 2 * (seqs // group),)),
        ],
        compiler_params=pltpu.CompilerParams(vmem_limit_bytes=36 * 2**20),
        name="attention",
    )(*in_hbm(lengths, tokens, norm_attn.reshape(1, -1), attn_bias, w_query, w_key,
              w_value, w_out, cache_keys, cache_values))


def middle_kernel(row_count, tokens_ref, keep_ref, got_ref, gain_ref, mix_ref, routes_ref,
                  weights_ref, out_ref, middle_ref, wide):
    width = keep_ref.shape[1]
    wide[...] = tokens_ref[...].astype(F32)
    own = pl.multiple_of(lax.axis_index("tp") * row_count, 8)
    attn_sum = keep_ref[...].astype(F32) + got_ref[...].astype(F32)
    middle = (wide[pl.ds(own, row_count), :] + attn_sum).astype(BF16)
    middle_ref[...] = middle
    normed = normed_block(middle.astype(F32), gain_ref[...])
    out_ref[:, :width] = normed
    dot = jnp.sum(normed.astype(F32) * mix_ref[...].astype(F32), axis=-1, keepdims=True)
    gate = 1.0 / (1.0 + jnp.exp(-dot))
    coarse = gate.astype(BF16).astype(F32)
    lane = lax.broadcasted_iota(jnp.int32, (row_count, LANES), 1)
    extra = jnp.where(lane == EXPERTS, coarse, 0.0)
    extra = jnp.where(lane == EXPERTS + 1, gate - coarse, extra)
    for choice in range(routes_ref.shape[1]):
        extra += jnp.where(
            lane == routes_ref[:, choice:choice + 1],
            weights_ref[:, choice:choice + 1].astype(F32), 0.0,
        )
    out_ref[:, width:] = extra.astype(BF16)


def make_middle(tokens, keep, got, norm_ffn, dense_mix, routes, route_weights):
    row_count, width = keep.shape
    return pl.pallas_call(
        functools.partial(middle_kernel, row_count),
        out_shape=(
            jax.ShapeDtypeStruct((row_count, width + LANES), BF16),
            jax.ShapeDtypeStruct((row_count, width), BF16),
        ),
        in_specs=[VMEM] * 7,
        out_specs=(VMEM,) * 2,
        scratch_shapes=[pltpu.VMEM(tokens.shape, F32)],
        compiler_params=pltpu.CompilerParams(vmem_limit_bytes=4 * 2**20),
        name="middle",
    )(tokens, keep, got, norm_ffn.reshape(1, -1), dense_mix.reshape(1, -1), routes,
      route_weights)


def units_part(units):
    return pl.ds(pl.multiple_of(lax.axis_index("tp") * units, 8), units)


def fetch_kernel(plan, count, *refs):
    sems = refs[-1]
    copies = [
        pltpu.make_async_copy(source, target, sems.at[i])
        for i, (source, target) in enumerate(plan(refs[1:1 + count], refs[1 + count:-1]))
    ]
    for copy in copies:
        copy.start()
    for copy in copies:
        copy.wait()


def fetch(after, arrays, shapes, copies, plan):
    size = sum(2 * math.prod(shape) for shape in shapes)
    return pl.pallas_call(
        functools.partial(fetch_kernel, plan, len(arrays)),
        out_shape=tuple(pltpu.VMEM(shape, BF16) for shape in shapes),
        in_specs=[HBM] * (1 + len(arrays)),
        out_specs=(VMEM,) * len(shapes),
        scratch_shapes=[pltpu.SemaphoreType.DMA((copies,))],
        cost_estimate=pl.CostEstimate(
            flops=FETCH_FLOPS * size, bytes_accessed=size, transcendentals=0
        ),
        compiler_params=pltpu.CompilerParams(vmem_limit_bytes=2**20),
    )(after, *in_hbm(*arrays))


def wide_plan(first, count, gate_hbm, up_hbm, target):
    pairs = []
    for i in range(count):
        cols = pl.ds((first + i) * BLOCK, BLOCK)
        pairs.append((gate_hbm.at[:, cols], target.at[i, :, pl.ds(0, BLOCK)]))
        pairs.append((up_hbm.at[:, cols], target.at[i, :, pl.ds(BLOCK, BLOCK)]))
    return pairs


def fetch_weights(after, expert_gate, expert_up, expert_down, dense_gate_w, dense_up_w,
                  dense_down_w):
    width, units = expert_gate.shape
    blocks = units // BLOCK
    early = 1
    joined = units % BLOCK == 0 and blocks > early
    dense_units = dense_gate_w.shape[1] // lax.axis_size("tp")

    def first_plan(sources, targets):
        part = units_part(dense_units)
        pairs = [
            (sources[i].at[part], target)
            for i, target in enumerate((targets[0].at[0], targets[0].at[1], targets[1]))
        ]
        if joined:
            return pairs + wide_plan(0, early, sources[3], sources[4], targets[2])
        return pairs + [(sources[3], targets[2].at[0])]

    def second_plan(sources, targets):
        half = units // 2
        return [
            (sources[0].at[pl.ds(i * half, half)], targets[0].at[pl.ds(i * half, half)])
            for i in range(2)
        ]

    def third_plan(sources, targets):
        if joined:
            return wide_plan(early, blocks - early, *sources, targets[0])
        return [(sources[1], targets[0].at[0])]

    dense, dense_down, first_wide = fetch(
        after[0],
        (dense_gate_w.T, dense_up_w.T, dense_down_w, expert_gate, expert_up),
        (
            (2, dense_units, width), (dense_units, width),
            (early, width, 2 * BLOCK) if joined else (1, width, units),
        ),
        3 + (2 * early if joined else 1), first_plan,
    )
    down, = fetch(after[1], (expert_down,), ((units, width),), 2, second_plan)
    last_wide, = fetch(
        after[2], (expert_gate, expert_up),
        ((blocks - early, width, 2 * BLOCK) if joined else (1, width, units),),
        2 * (blocks - early) if joined else 1, third_plan,
    )
    return first_wide, last_wide, dense, down, dense_down


def ffn_kernel(members, out_block, rows_ref, first_wide, last_wide, dense, down, dense_down,
               own_ref, other_ref, hidden_ref):
    count, padded = rows_ref.shape
    width = padded - LANES
    units = down.shape[0]
    device = lax.axis_index("ep") * lax.axis_size("tp") + lax.axis_index("tp")
    expert = device // members
    extra = rows_ref[:, width:].astype(F32)
    lane = lax.broadcasted_iota(jnp.int32, extra.shape, 1)
    share = jnp.sum(jnp.where(lane == expert, extra, 0.0), axis=-1, keepdims=True)
    gated = (lane == EXPERTS) | (lane == EXPERTS + 1)
    mix = jnp.sum(jnp.where(gated, extra, 0.0), axis=-1, keepdims=True)

    def activate(gate, up, scale):
        return (gate / (1.0 + jnp.exp(-gate)) * up * scale).astype(BF16)

    rows = rows_ref[:, :width]
    if first_wide.shape[2] == units:
        gate = jnp.dot(rows, first_wide[0], preferred_element_type=F32)
        up = jnp.dot(rows, last_wide[0], preferred_element_type=F32)
        hidden_ref[...] = activate(gate, up, share)
    else:
        early = first_wide.shape[0]
        for i in range(units // BLOCK):
            weights = first_wide[i] if i < early else last_wide[i - early]
            both = jnp.dot(rows, weights, preferred_element_type=F32)
            hidden_ref[:, i * BLOCK:(i + 1) * BLOCK] = activate(
                both[:, :BLOCK], both[:, BLOCK:], share
            )
    dims = (((1,), (1,)), ((), ()))
    gate, up = (
        lax.dot_general(rows, dense[i], dims, preferred_element_type=F32) for i in range(2)
    )
    dense_hidden = activate(gate, up, mix)
    for first in range(0, width, out_block):
        cols = slice(first, first + out_block)
        total = jnp.dot(hidden_ref[...], down[:, cols], preferred_element_type=F32)
        total += jnp.dot(dense_hidden, dense_down[:, cols], preferred_element_type=F32)
        own_ref[:, cols] = total[:count // 2]
        other_ref[:, cols] = total[count // 2:].astype(BF16)


def feed_forward(rows, weights, members):
    count, padded = rows.shape
    width = padded - LANES
    units = weights[3].shape[0]
    return pl.pallas_call(
        functools.partial(ffn_kernel, members, 512 if width % 512 == 0 else width),
        out_shape=(
            jax.ShapeDtypeStruct((count // 2, width), F32),
            jax.ShapeDtypeStruct((count // 2, width), BF16),
        ),
        in_specs=[VMEM] * 6,
        out_specs=(VMEM,) * 2,
        scratch_shapes=[pltpu.VMEM((count, units), BF16)],
        cost_estimate=pl.CostEstimate(
            flops=6 * count * width * units, bytes_accessed=0, transcendentals=0
        ),
        compiler_params=pltpu.CompilerParams(vmem_limit_bytes=16 * 2**20),
        name="feed_forward",
    )(rows, *weights)


def phases_of(n_ep):
    bits = [1 << b for b in range(n_ep.bit_length() - 1)]
    doublings = []
    while len(bits) >= 4:
        high, low = bits.pop(), bits.pop()
        doublings += [(high, low), (low, high)]
    doublings += [(bit, bit) for bit in bits[2:]]
    direct = [(2, 1), (1, 2), (3, 3)] if len(bits) >= 2 else [(bit, bit) for bit in bits]
    return doublings, direct


def exchange(array, masks, n_ep, n_tp):
    pairs = [
        (ep * n_tp + tp, (ep ^ masks[tp % 2]) * n_tp + tp)
        for ep in range(n_ep) for tp in range(n_tp)
    ]
    return lax.ppermute(array, ("ep", "tp"), pairs)


def swap(array, n_tp):
    return lax.ppermute(array, "tp", [(i, i ^ 1) for i in range(n_tp)])


def layer(
    tokens, norm_attn, w_query, w_key, w_value, w_out, attn_bias, cache_keys, cache_values,
    lengths, norm_ffn, expert_gate, expert_up, expert_down, dense_gate_w, dense_up_w,
    dense_down_w, dense_mix, routes, route_weights,
):
    n_ep, n_tp = lax.axis_size("ep"), lax.axis_size("tp")
    row_count = tokens.shape[0] // n_tp
    keep, send, new_keys, new_values = attention(
        tokens, norm_attn, w_query, w_key, w_value, w_out, attn_bias, cache_keys,
        cache_values, lengths, row_count,
    )
    rows, middle = make_middle(
        tokens, keep, swap(send, n_tp), norm_ffn, dense_mix, routes, route_weights
    )
    doublings, direct = phases_of(n_ep)
    held = []
    for masks in doublings:
        held.append(rows)
        got = exchange(rows, masks, n_ep, n_tp)
        rows = jnp.concatenate([rows, got], axis=0)
    pieces = [rows]
    for masks in direct:
        pieces.append(exchange(rows, masks, n_ep, n_tp))
    weights = fetch_weights(
        (held[-2], held[-1], rows), expert_gate, expert_up, expert_down, dense_gate_w,
        dense_up_w, dense_down_w,
    )
    rows = jnp.concatenate(pieces, axis=0)
    rows = jnp.concatenate([rows, swap(rows, n_tp)], axis=0)
    own, other = feed_forward(rows, weights, n_ep * n_tp // EXPERTS)
    total = own + swap(other, n_tp).astype(F32)
    part = total.shape[0] // (len(direct) + 1)
    sent = [
        exchange(total[(i + 1) * part:(i + 2) * part].astype(BF16), masks, n_ep, n_tp)
        for i, masks in enumerate(direct)
    ]
    total = total[:part]
    for got in sent:
        total = total + got.astype(F32)
    for masks in reversed(doublings):
        half = total.shape[0] // 2
        got = exchange(total[half:].astype(BF16), masks, n_ep, n_tp)
        total = total[:half] + got.astype(F32)
    layer_out = (middle.astype(F32) + total).astype(BF16)
    return layer_out, new_keys, new_values


def solution(mesh):
    placed = (
        P("ep", None),
        P(),
        P(None, "tp"),
        P(None, "tp"),
        P(None, "tp"),
        P("tp", None),
        P("tp"),
        P("ep", None, "tp"),
        P("ep", None, "tp"),
        P("ep"),
        P(),
        P(None, ("ep", "tp")),
        P(None, ("ep", "tp")),
        P(("ep", "tp"), None),
        P(None, "ep"),
        P(None, "ep"),
        P("ep", None),
        P(),
        P(("ep", "tp"), None),
        P(("ep", "tp"), None),
    )
    return jax.shard_map(
        layer,
        mesh=mesh,
        in_specs=placed,
        out_specs=(P(("ep", "tp"), None), P("ep", "tp"), P("ep", "tp")),
        check_vma=False,
    )
```

```python
import functools
import math

import jax
import jax.numpy as jnp
from jax import lax
from jax.experimental import pallas as pl
from jax.experimental.pallas import tpu as pltpu
from jax.sharding import PartitionSpec as P

HEAD_DIM = 64
EXPERTS = 8
LANES = 128
BLOCK = 256
EPSILON = 1e-06
FETCH_FLOPS = 200
IN_FLIGHT = 8
GROUP = 8
F32 = jnp.float32
BF16 = jnp.bfloat16


HBM = pl.BlockSpec(memory_space=pltpu.HBM)
VMEM = pl.BlockSpec(memory_space=pltpu.VMEM)


def in_hbm(*arrays):
    return [pltpu.with_memory_space_constraint(array, pltpu.HBM) for array in arrays]


def split_of(total, most):
    for pieces in range(most, 0, -1):
        if total % (pieces * 256) == 0:
            return pieces
    return 1


def normed_block(widened, gain):
    scale = lax.rsqrt(jnp.mean(widened * widened, axis=-1, keepdims=True) + EPSILON)
    return (widened * scale * gain).astype(BF16)


def attention_kernel(
    row_count, group, q_parts, o_parts,
    lengths_hbm, tokens_hbm, gain_hbm, bias_hbm,
    wq_hbm, wk_hbm, wv_hbm, wo_hbm, keys_hbm, values_hbm,
    keep_ref, send_ref, new_keys_ref, new_values_ref,
    lengths_ref, tokens_ref, gain_ref, bias_ref,
    wq, wk, wv, wo, keys, values, queries, mixed, later, partial,
    sems,
):
    seqs, width = tokens_ref.shape
    cache = keys.shape[1]
    q_width = wq.shape[1]
    heads = q_width // HEAD_DIM
    pairs = heads // 2
    groups = seqs // group
    q_rows = width // q_parts
    o_rows = q_width // o_parts
    half = 2 * LANES

    plan = [
        (tokens_hbm, tokens_ref), (gain_hbm, gain_ref), (lengths_hbm, lengths_ref),
        (bias_hbm, bias_ref),
    ]
    small = len(plan)
    for i in range(q_parts):
        part = pl.ds(i * q_rows, q_rows)
        plan.append((wq_hbm.at[part], wq.at[part]))
    parts = [pl.ds(i * group, group) for i in range(groups)]
    plan.append((keys_hbm.at[parts[0]], keys.at[parts[0]]))
    for i in range(groups):
        for part in parts[i + 1:i + 2]:
            plan.append((keys_hbm.at[part], keys.at[part]))
        plan.append((values_hbm.at[parts[i]], values.at[parts[i]]))
    plan += [(wk_hbm, wk), (wv_hbm, wv)]
    for i in range(o_parts):
        part = pl.ds(i * o_rows, o_rows)
        plan.append((wo_hbm.at[part], wo.at[part]))
    copies = [
        pltpu.make_async_copy(source, target, sems.at[i])
        for i, (source, target) in enumerate(plan)
    ]
    waited = [0]
    for copy in copies[:small + IN_FLIGHT]:
        copy.start()

    def arrive(count):
        for _ in range(count):
            copies[waited[0]].wait()
            waited[0] += 1
            following = waited[0] + IN_FLIGHT - 1
            if waited[0] > small and following < len(copies):
                copies[following].start()

    later_rows = lax.broadcasted_iota(jnp.int32, (2 * half, half), 0) % half
    later_cols = lax.broadcasted_iota(jnp.int32, (2 * half, half), 1)
    later[...] = (later_rows > later_cols).astype(F32).astype(BF16)

    arrive(small)
    normed = normed_block(tokens_ref[...].astype(F32), gain_ref[...])
    query = jnp.zeros((seqs, q_width), F32)
    for i in range(q_parts):
        arrive(1)
        query += jnp.dot(
            normed[:, i * q_rows:(i + 1) * q_rows],
            wq[i * q_rows:(i + 1) * q_rows, :],
            preferred_element_type=F32,
        )
    query = query.astype(BF16).astype(F32)

    lane = lax.broadcasted_iota(jnp.int32, (seqs, LANES), 1)
    low = lane < HEAD_DIM
    for pair in range(pairs):
        both = query[:, pair * LANES:(pair + 1) * LANES]
        turned = pltpu.roll(both, HEAD_DIM, 1)
        if 2 * pair < heads // 2:
            first, second = jnp.where(low, both, 0.0), jnp.where(low, turned, 0.0)
        else:
            first, second = jnp.where(low, 0.0, turned), jnp.where(low, 0.0, both)
        queries[pl.ds(2 * pair, seqs, stride=heads), :] = first
        queries[pl.ds(2 * pair + 1, seqs, stride=heads), :] = second

    rows = group * heads
    head_of = lax.broadcasted_iota(jnp.int32, (heads, 1), 0)
    bias = jnp.zeros((heads, 1), F32)
    for head in range(heads):
        bias = jnp.where(head_of == head, bias_ref[head], bias)
    bias = jnp.concatenate([bias] * group, axis=0)
    seq_of = lax.broadcasted_iota(jnp.int32, (rows, 1), 0) // heads
    place = lax.broadcasted_iota(jnp.int32, (rows, half), 1)
    blocks = cache // half

    def score(step):
        arrive(1)
        scores = []
        for s in range(step * group, (step + 1) * group):
            q_seq = queries[pl.ds(s * heads, heads), :].astype(BF16)
            scores.append(
                lax.dot_general(
                    q_seq, keys[s], (((1,), (1,)), ((), ())), preferred_element_type=F32
                )
            )
        return jnp.concatenate(scores, axis=0)

    def weigh(step, scores):
        length = jnp.zeros((rows, 1), jnp.int32)
        for s in range(group):
            length = jnp.where(seq_of == s, lengths_ref[step * group + s], length)
        opened, pieces, heads_first = [], [], []
        for n in range(blocks):
            z = scores[:, n * half:(n + 1) * half] * HEAD_DIM ** (-0.5) + bias
            shared = jnp.log(1.0 + jnp.exp(-jnp.abs(z)))
            visible = place + n * half < length
            kept = jnp.where(visible, -(jnp.maximum(z, 0.0) + shared), 0.0)
            opened.append(jnp.where(visible, jnp.minimum(z, 0.0) - shared, -jnp.inf))
            coarse = kept.astype(BF16)
            fine = (kept - coarse.astype(F32)).astype(BF16)
            pieces.append(jnp.concatenate([coarse, fine], axis=1))
            heads_first.append(kept[:, 0:1])
        after = jnp.dot(
            jnp.concatenate(pieces, axis=0), later[...], preferred_element_type=F32
        )
        beyond = jnp.zeros((rows, 1), F32)
        weights = [None] * blocks
        for n in reversed(range(blocks)):
            within = after[n * rows:(n + 1) * rows]
            weights[n] = jnp.exp(opened[n] + within + beyond).astype(BF16)
            beyond = beyond + within[:, 0:1] + heads_first[n]
        return jnp.concatenate(weights, axis=1)

    def mix(step, weights):
        arrive(1)
        for s in range(group):
            seq = step * group + s
            mixed[pl.ds(seq * heads, heads), :] = jnp.dot(
                weights[s * heads:(s + 1) * heads], values[seq], preferred_element_type=F32
            )

    scores = score(0)
    for step in range(groups):
        following = score(step + 1) if step + 1 < groups else None
        weights = weigh(step, scores)
        mix(step, weights)
        scores = following

    arrive(2)
    new_keys_ref[...] = jnp.dot(normed, wk[...], preferred_element_type=F32).astype(BF16)
    new_values_ref[...] = jnp.dot(normed, wv[...], preferred_element_type=F32).astype(BF16)

    joined = []
    for pair in range(pairs):
        first = mixed[pl.ds(2 * pair, seqs, stride=heads), :]
        second = mixed[pl.ds(2 * pair + 1, seqs, stride=heads), :]
        if 2 * pair < heads // 2:
            second = pltpu.roll(second, HEAD_DIM, 1)
        else:
            first = pltpu.roll(first, HEAD_DIM, 1)
        joined.append(jnp.where(low, first, second).astype(BF16))
    heads_out = jnp.concatenate(joined, axis=1)
    total = jnp.zeros((seqs, width), F32)
    for i in range(o_parts):
        arrive(1)
        total += jnp.dot(
            heads_out[:, i * o_rows:(i + 1) * o_rows],
            wo[i * o_rows:(i + 1) * o_rows, :],
            preferred_element_type=F32,
        )
    partial[...] = total
    own = lax.axis_index("tp") * row_count
    other = seqs - row_count - own
    keep_ref[...] = partial[pl.ds(pl.multiple_of(own, 8), row_count), :].astype(BF16)
    send_ref[...] = partial[pl.ds(pl.multiple_of(other, 8), row_count), :].astype(BF16)


def attention(tokens, norm_attn, w_query, w_key, w_value, w_out, attn_bias,
              cache_keys, cache_values, lengths, row_count):
    seqs, width = tokens.shape
    q_width = w_query.shape[1]
    kv_width = w_key.shape[1]
    heads = q_width // HEAD_DIM
    group = GROUP if seqs % GROUP == 0 else 1
    q_parts = split_of(width, 4)
    o_parts = split_of(q_width, 4)
    dma = pltpu.SemaphoreType.DMA
    half = jax.ShapeDtypeStruct((row_count, width), BF16)
    kv = jax.ShapeDtypeStruct((seqs, kv_width), BF16)
    return pl.pallas_call(
        functools.partial(attention_kernel, row_count, group, q_parts, o_parts),
        out_shape=(half, half, kv, kv),
        in_specs=[HBM] * 10,
        out_specs=(VMEM,) * 4,
        scratch_shapes=[
            pltpu.SMEM(lengths.shape, jnp.int32),
            pltpu.VMEM(tokens.shape, BF16),
            pltpu.VMEM((1, width), F32),
            pltpu.SMEM(attn_bias.shape, F32),
            pltpu.VMEM(w_query.shape, BF16),
            pltpu.VMEM(w_key.shape, BF16),
            pltpu.VMEM(w_value.shape, BF16),
            pltpu.VMEM(w_out.shape, BF16),
            pltpu.VMEM(cache_keys.shape, BF16),
            pltpu.VMEM(cache_values.shape, BF16),
            pltpu.VMEM((seqs * heads, LANES), F32),
            pltpu.VMEM((seqs * heads, LANES), F32),
            pltpu.VMEM((4 * LANES, 2 * LANES), BF16),
            pltpu.VMEM((seqs, width), F32),
            dma((6 + q_parts + o_parts + 2 * (seqs // group),)),
        ],
        compiler_params=pltpu.CompilerParams(vmem_limit_bytes=36 * 2**20),
        name="attention",
    )(*in_hbm(lengths, tokens, norm_attn.reshape(1, -1), attn_bias, w_query, w_key,
              w_value, w_out, cache_keys, cache_values))


def middle_kernel(row_count, tokens_ref, keep_ref, got_ref, gain_ref, mix_ref, routes_ref,
                  weights_ref, out_ref, middle_ref, wide):
    width = keep_ref.shape[1]
    wide[...] = tokens_ref[...].astype(F32)
    own = pl.multiple_of(lax.axis_index("tp") * row_count, 8)
    attn_sum = keep_ref[...].astype(F32) + got_ref[...].astype(F32)
    middle = (wide[pl.ds(own, row_count), :] + attn_sum).astype(BF16)
    middle_ref[...] = middle
    normed = normed_block(middle.astype(F32), gain_ref[...])
    out_ref[:, :width] = normed
    dot = jnp.sum(normed.astype(F32) * mix_ref[...].astype(F32), axis=-1, keepdims=True)
    gate = 1.0 / (1.0 + jnp.exp(-dot))
    coarse = gate.astype(BF16).astype(F32)
    lane = lax.broadcasted_iota(jnp.int32, (row_count, LANES), 1)
    extra = jnp.where(lane == EXPERTS, coarse, 0.0)
    extra = jnp.where(lane == EXPERTS + 1, gate - coarse, extra)
    for choice in range(routes_ref.shape[1]):
        extra += jnp.where(
            lane == routes_ref[:, choice:choice + 1],
            weights_ref[:, choice:choice + 1].astype(F32), 0.0,
        )
    out_ref[:, width:] = extra.astype(BF16)


def make_middle(tokens, keep, got, norm_ffn, dense_mix, routes, route_weights):
    row_count, width = keep.shape
    return pl.pallas_call(
        functools.partial(middle_kernel, row_count),
        out_shape=(
            jax.ShapeDtypeStruct((row_count, width + LANES), BF16),
            jax.ShapeDtypeStruct((row_count, width), BF16),
        ),
        in_specs=[VMEM] * 7,
        out_specs=(VMEM,) * 2,
        scratch_shapes=[pltpu.VMEM(tokens.shape, F32)],
        compiler_params=pltpu.CompilerParams(vmem_limit_bytes=4 * 2**20),
        name="middle",
    )(tokens, keep, got, norm_ffn.reshape(1, -1), dense_mix.reshape(1, -1), routes,
      route_weights)


def units_part(units):
    return pl.ds(pl.multiple_of(lax.axis_index("tp") * units, 8), units)


def fetch_kernel(plan, count, *refs):
    sems = refs[-1]
    copies = [
        pltpu.make_async_copy(source, target, sems.at[i])
        for i, (source, target) in enumerate(plan(refs[1:1 + count], refs[1 + count:-1]))
    ]
    for copy in copies:
        copy.start()
    for copy in copies:
        copy.wait()


def fetch(after, arrays, shapes, copies, plan):
    size = sum(2 * math.prod(shape) for shape in shapes)
    return pl.pallas_call(
        functools.partial(fetch_kernel, plan, len(arrays)),
        out_shape=tuple(pltpu.VMEM(shape, BF16) for shape in shapes),
        in_specs=[HBM] * (1 + len(arrays)),
        out_specs=(VMEM,) * len(shapes),
        scratch_shapes=[pltpu.SemaphoreType.DMA((copies,))],
        cost_estimate=pl.CostEstimate(
            flops=FETCH_FLOPS * size, bytes_accessed=size, transcendentals=0
        ),
        compiler_params=pltpu.CompilerParams(vmem_limit_bytes=2**20),
    )(after, *in_hbm(*arrays))


def wide_plan(first, count, gate_hbm, up_hbm, target):
    pairs = []
    for i in range(count):
        cols = pl.ds((first + i) * BLOCK, BLOCK)
        pairs.append((gate_hbm.at[:, cols], target.at[i, :, pl.ds(0, BLOCK)]))
        pairs.append((up_hbm.at[:, cols], target.at[i, :, pl.ds(BLOCK, BLOCK)]))
    return pairs


def fetch_weights(after, expert_gate, expert_up, expert_down, dense_gate_w, dense_up_w,
                  dense_down_w):
    width, units = expert_gate.shape
    blocks = units // BLOCK
    early = 1
    joined = units % BLOCK == 0 and blocks > early
    dense_units = dense_gate_w.shape[1] // lax.axis_size("tp")

    def first_plan(sources, targets):
        part = units_part(dense_units)
        pairs = [
            (sources[i].at[part], target)
            for i, target in enumerate((targets[0].at[0], targets[0].at[1], targets[1]))
        ]
        if joined:
            return pairs + wide_plan(0, early, sources[3], sources[4], targets[2])
        return pairs + [(sources[3], targets[2].at[0])]

    def second_plan(sources, targets):
        half = units // 2
        return [
            (sources[0].at[pl.ds(i * half, half)], targets[0].at[pl.ds(i * half, half)])
            for i in range(2)
        ]

    def third_plan(sources, targets):
        if joined:
            return wide_plan(early, blocks - early, *sources, targets[0])
        return [(sources[1], targets[0].at[0])]

    dense, dense_down, first_wide = fetch(
        after[0],
        (dense_gate_w.T, dense_up_w.T, dense_down_w, expert_gate, expert_up),
        (
            (2, dense_units, width), (dense_units, width),
            (early, width, 2 * BLOCK) if joined else (1, width, units),
        ),
        3 + (2 * early if joined else 1), first_plan,
    )
    down, = fetch(after[1], (expert_down,), ((units, width),), 2, second_plan)
    last_wide, = fetch(
        after[2], (expert_gate, expert_up),
        ((blocks - early, width, 2 * BLOCK) if joined else (1, width, units),),
        2 * (blocks - early) if joined else 1, third_plan,
    )
    return first_wide, last_wide, dense, down, dense_down


def ffn_kernel(members, out_block, rows_ref, first_wide, last_wide, dense, down, dense_down,
               own_ref, other_ref, hidden_ref):
    count, padded = rows_ref.shape
    width = padded - LANES
    units = down.shape[0]
    device = lax.axis_index("ep") * lax.axis_size("tp") + lax.axis_index("tp")
    expert = device // members
    extra = rows_ref[:, width:].astype(F32)
    lane = lax.broadcasted_iota(jnp.int32, extra.shape, 1)
    share = jnp.sum(jnp.where(lane == expert, extra, 0.0), axis=-1, keepdims=True)
    gated = (lane == EXPERTS) | (lane == EXPERTS + 1)
    mix = jnp.sum(jnp.where(gated, extra, 0.0), axis=-1, keepdims=True)

    def activate(gate, up, scale):
        return (gate / (1.0 + jnp.exp(-gate)) * up * scale).astype(BF16)

    rows = rows_ref[:, :width]
    if first_wide.shape[2] == units:
        gate = jnp.dot(rows, first_wide[0], preferred_element_type=F32)
        up = jnp.dot(rows, last_wide[0], preferred_element_type=F32)
        hidden_ref[...] = activate(gate, up, share)
    else:
        early = first_wide.shape[0]
        for i in range(units // BLOCK):
            weights = first_wide[i] if i < early else last_wide[i - early]
            both = jnp.dot(rows, weights, preferred_element_type=F32)
            hidden_ref[:, i * BLOCK:(i + 1) * BLOCK] = activate(
                both[:, :BLOCK], both[:, BLOCK:], share
            )
    dims = (((1,), (1,)), ((), ()))
    gate, up = (
        lax.dot_general(rows, dense[i], dims, preferred_element_type=F32) for i in range(2)
    )
    dense_hidden = activate(gate, up, mix)
    for first in range(0, width, out_block):
        cols = slice(first, first + out_block)
        total = jnp.dot(hidden_ref[...], down[:, cols], preferred_element_type=F32)
        total += jnp.dot(dense_hidden, dense_down[:, cols], preferred_element_type=F32)
        own_ref[:, cols] = total[:count // 2]
        other_ref[:, cols] = total[count // 2:].astype(BF16)


def feed_forward(rows, weights, members):
    count, padded = rows.shape
    width = padded - LANES
    units = weights[3].shape[0]
    return pl.pallas_call(
        functools.partial(ffn_kernel, members, 512 if width % 512 == 0 else width),
        out_shape=(
            jax.ShapeDtypeStruct((count // 2, width), F32),
            jax.ShapeDtypeStruct((count // 2, width), BF16),
        ),
        in_specs=[VMEM] * 6,
        out_specs=(VMEM,) * 2,
        scratch_shapes=[pltpu.VMEM((count, units), BF16)],
        cost_estimate=pl.CostEstimate(
            flops=6 * count * width * units, bytes_accessed=0, transcendentals=0
        ),
        compiler_params=pltpu.CompilerParams(vmem_limit_bytes=16 * 2**20),
        name="feed_forward",
    )(rows, *weights)


def phases_of(n_ep):
    bits = [1 << b for b in range(n_ep.bit_length() - 1)]
    doublings = []
    while len(bits) >= 4:
        high, low = bits.pop(), bits.pop()
        doublings += [(high, low), (low, high)]
    doublings += [(bit, bit) for bit in bits[2:]]
    direct = [(2, 1), (1, 2), (3, 3)] if len(bits) >= 2 else [(bit, bit) for bit in bits]
    return doublings, direct


def exchange(array, masks, n_ep, n_tp):
    pairs = [
        (ep * n_tp + tp, (ep ^ masks[tp % 2]) * n_tp + tp)
        for ep in range(n_ep) for tp in range(n_tp)
    ]
    return lax.ppermute(array, ("ep", "tp"), pairs)


def swap(array, n_tp):
    return lax.ppermute(array, "tp", [(i, i ^ 1) for i in range(n_tp)])


def layer(
    tokens, norm_attn, w_query, w_key, w_value, w_out, attn_bias, cache_keys, cache_values,
    lengths, norm_ffn, expert_gate, expert_up, expert_down, dense_gate_w, dense_up_w,
    dense_down_w, dense_mix, routes, route_weights,
):
    n_ep, n_tp = lax.axis_size("ep"), lax.axis_size("tp")
    row_count = tokens.shape[0] // n_tp
    keep, send, new_keys, new_values = attention(
        tokens, norm_attn, w_query, w_key, w_value, w_out, attn_bias, cache_keys,
        cache_values, lengths, row_count,
    )
    rows, middle = make_middle(
        tokens, keep, swap(send, n_tp), norm_ffn, dense_mix, routes, route_weights
    )
    doublings, direct = phases_of(n_ep)
    held = []
    for masks in doublings:
        held.append(rows)
        got = exchange(rows, masks, n_ep, n_tp)
        rows = jnp.concatenate([rows, got], axis=0)
    pieces = [rows]
    for masks in direct:
        pieces.append(exchange(rows, masks, n_ep, n_tp))
    weights = fetch_weights(
        (held[-2], held[-1], rows), expert_gate, expert_up, expert_down, dense_gate_w,
        dense_up_w, dense_down_w,
    )
    rows = jnp.concatenate(pieces, axis=0)
    rows = jnp.concatenate([rows, swap(rows, n_tp)], axis=0)
    own, other = feed_forward(rows, weights, n_ep * n_tp // EXPERTS)
    total = own + swap(other, n_tp).astype(F32)
    part = total.shape[0] // (2 * (len(direct) + 1))
    sums = []
    for side in (1, 0):
        sent = [
            exchange(
                total[(2 * i + 2 + side) * part:(2 * i + 3 + side) * part].astype(BF16),
                masks, n_ep, n_tp,
            )
            for i, masks in enumerate(direct)
        ]
        summed = total[side * part:(side + 1) * part]
        for got in sent:
            summed = summed + got.astype(F32)
        sums.append(summed)
    second, total = sums
    got = exchange(second.astype(BF16), doublings[-1], n_ep, n_tp)
    total = total + got.astype(F32)
    for masks in reversed(doublings[:-1]):
        half = total.shape[0] // 2
        got = exchange(total[half:].astype(BF16), masks, n_ep, n_tp)
        total = total[:half] + got.astype(F32)
    layer_out = (middle.astype(F32) + total).astype(BF16)
    return layer_out, new_keys, new_values


def solution(mesh):
    placed = (
        P("ep", None),
        P(),
        P(None, "tp"),
        P(None, "tp"),
        P(None, "tp"),
        P("tp", None),
        P("tp"),
        P("ep", None, "tp"),
        P("ep", None, "tp"),
        P("ep"),
        P(),
        P(None, ("ep", "tp")),
        P(None, ("ep", "tp")),
        P(("ep", "tp"), None),
        P(None, "ep"),
        P(None, "ep"),
        P("ep", None),
        P(),
        P(("ep", "tp"), None),
        P(("ep", "tp"), None),
    )
    return jax.shard_map(
        layer,
        mesh=mesh,
        in_specs=placed,
        out_specs=(P(("ep", "tp"), None), P("ep", "tp"), P("ep", "tp")),
        check_vma=False,
    )
```

```python
import functools
import math

import jax
import jax.numpy as jnp
from jax import lax
from jax.experimental import pallas as pl
from jax.experimental.pallas import tpu as pltpu
from jax.sharding import PartitionSpec as P

HEAD_DIM = 64
EXPERTS = 8
LANES = 128
BLOCK = 256
LAST = 1
EPSILON = 1e-06
FETCH_FLOPS = 200
IN_FLIGHT = 8
GROUP = 8
F32 = jnp.float32
BF16 = jnp.bfloat16


HBM = pl.BlockSpec(memory_space=pltpu.HBM)
VMEM = pl.BlockSpec(memory_space=pltpu.VMEM)


def in_hbm(*arrays):
    return [pltpu.with_memory_space_constraint(array, pltpu.HBM) for array in arrays]


def split_of(total, most):
    for pieces in range(most, 0, -1):
        if total % (pieces * 256) == 0:
            return pieces
    return 1


def normed_block(widened, gain):
    scale = lax.rsqrt(jnp.mean(widened * widened, axis=-1, keepdims=True) + EPSILON)
    return (widened * scale * gain).astype(BF16)


def attention_kernel(
    row_count, group, q_parts, o_parts,
    lengths_hbm, tokens_hbm, gain_hbm, bias_hbm,
    wq_hbm, wk_hbm, wv_hbm, wo_hbm, keys_hbm, values_hbm,
    keep_ref, send_ref, new_keys_ref, new_values_ref,
    lengths_ref, tokens_ref, gain_ref, bias_ref,
    wq, wk, wv, wo, keys, values, queries, mixed, later, partial,
    sems,
):
    seqs, width = tokens_ref.shape
    cache = keys.shape[1]
    q_width = wq.shape[1]
    heads = q_width // HEAD_DIM
    pairs = heads // 2
    groups = seqs // group
    q_rows = width // q_parts
    o_rows = q_width // o_parts
    half = 2 * LANES

    plan = [
        (tokens_hbm, tokens_ref), (gain_hbm, gain_ref), (lengths_hbm, lengths_ref),
        (bias_hbm, bias_ref),
    ]
    small = len(plan)
    for i in range(q_parts):
        part = pl.ds(i * q_rows, q_rows)
        plan.append((wq_hbm.at[part], wq.at[part]))
    parts = [pl.ds(i * group, group) for i in range(groups)]
    plan.append((keys_hbm.at[parts[0]], keys.at[parts[0]]))
    for i in range(groups):
        for part in parts[i + 1:i + 2]:
            plan.append((keys_hbm.at[part], keys.at[part]))
        plan.append((values_hbm.at[parts[i]], values.at[parts[i]]))
    plan += [(wk_hbm, wk), (wv_hbm, wv)]
    for i in range(o_parts):
        part = pl.ds(i * o_rows, o_rows)
        plan.append((wo_hbm.at[part], wo.at[part]))
    copies = [
        pltpu.make_async_copy(source, target, sems.at[i])
        for i, (source, target) in enumerate(plan)
    ]
    waited = [0]
    for copy in copies[:small + IN_FLIGHT]:
        copy.start()

    def arrive(count):
        for _ in range(count):
            copies[waited[0]].wait()
            waited[0] += 1
            following = waited[0] + IN_FLIGHT - 1
            if waited[0] > small and following < len(copies):
                copies[following].start()

    later_rows = lax.broadcasted_iota(jnp.int32, (2 * half, half), 0) % half
    later_cols = lax.broadcasted_iota(jnp.int32, (2 * half, half), 1)
    later[...] = (later_rows > later_cols).astype(F32).astype(BF16)

    arrive(small)
    normed = normed_block(tokens_ref[...].astype(F32), gain_ref[...])
    query = jnp.zeros((seqs, q_width), F32)
    for i in range(q_parts):
        arrive(1)
        query += jnp.dot(
            normed[:, i * q_rows:(i + 1) * q_rows],
            wq[i * q_rows:(i + 1) * q_rows, :],
            preferred_element_type=F32,
        )
    query = query.astype(BF16).astype(F32)

    lane = lax.broadcasted_iota(jnp.int32, (seqs, LANES), 1)
    low = lane < HEAD_DIM
    for pair in range(pairs):
        both = query[:, pair * LANES:(pair + 1) * LANES]
        turned = pltpu.roll(both, HEAD_DIM, 1)
        if 2 * pair < heads // 2:
            first, second = jnp.where(low, both, 0.0), jnp.where(low, turned, 0.0)
        else:
            first, second = jnp.where(low, 0.0, turned), jnp.where(low, 0.0, both)
        queries[pl.ds(2 * pair, seqs, stride=heads), :] = first
        queries[pl.ds(2 * pair + 1, seqs, stride=heads), :] = second

    rows = group * heads
    head_of = lax.broadcasted_iota(jnp.int32, (heads, 1), 0)
    bias = jnp.zeros((heads, 1), F32)
    for head in range(heads):
        bias = jnp.where(head_of == head, bias_ref[head], bias)
    bias = jnp.concatenate([bias] * group, axis=0)
    seq_of = lax.broadcasted_iota(jnp.int32, (rows, 1), 0) // heads
    place = lax.broadcasted_iota(jnp.int32, (rows, half), 1)
    blocks = cache // half

    def score(step):
        arrive(1)
        scores = []
        for s in range(step * group, (step + 1) * group):
            q_seq = queries[pl.ds(s * heads, heads), :].astype(BF16)
            scores.append(
                lax.dot_general(
                    q_seq, keys[s], (((1,), (1,)), ((), ())), preferred_element_type=F32
                )
            )
        return jnp.concatenate(scores, axis=0)

    def weigh(step, scores):
        length = jnp.zeros((rows, 1), jnp.int32)
        for s in range(group):
            length = jnp.where(seq_of == s, lengths_ref[step * group + s], length)
        opened, pieces, heads_first = [], [], []
        for n in range(blocks):
            z = scores[:, n * half:(n + 1) * half] * HEAD_DIM ** (-0.5) + bias
            shared = jnp.log(1.0 + jnp.exp(-jnp.abs(z)))
            visible = place + n * half < length
            kept = jnp.where(visible, -(jnp.maximum(z, 0.0) + shared), 0.0)
            opened.append(jnp.where(visible, jnp.minimum(z, 0.0) - shared, -jnp.inf))
            coarse = kept.astype(BF16)
            fine = (kept - coarse.astype(F32)).astype(BF16)
            pieces.append(jnp.concatenate([coarse, fine], axis=1))
            heads_first.append(kept[:, 0:1])
        after = jnp.dot(
            jnp.concatenate(pieces, axis=0), later[...], preferred_element_type=F32
        )
        beyond = jnp.zeros((rows, 1), F32)
        weights = [None] * blocks
        for n in reversed(range(blocks)):
            within = after[n * rows:(n + 1) * rows]
            weights[n] = jnp.exp(opened[n] + within + beyond).astype(BF16)
            beyond = beyond + within[:, 0:1] + heads_first[n]
        return jnp.concatenate(weights, axis=1)

    def mix(step, weights):
        arrive(1)
        for s in range(group):
            seq = step * group + s
            mixed[pl.ds(seq * heads, heads), :] = jnp.dot(
                weights[s * heads:(s + 1) * heads], values[seq], preferred_element_type=F32
            )

    scores = score(0)
    for step in range(groups):
        following = score(step + 1) if step + 1 < groups else None
        weights = weigh(step, scores)
        mix(step, weights)
        scores = following

    arrive(2)
    new_keys_ref[...] = jnp.dot(normed, wk[...], preferred_element_type=F32).astype(BF16)
    new_values_ref[...] = jnp.dot(normed, wv[...], preferred_element_type=F32).astype(BF16)

    joined = []
    for pair in range(pairs):
        first = mixed[pl.ds(2 * pair, seqs, stride=heads), :]
        second = mixed[pl.ds(2 * pair + 1, seqs, stride=heads), :]
        if 2 * pair < heads // 2:
            second = pltpu.roll(second, HEAD_DIM, 1)
        else:
            first = pltpu.roll(first, HEAD_DIM, 1)
        joined.append(jnp.where(low, first, second).astype(BF16))
    heads_out = jnp.concatenate(joined, axis=1)
    total = jnp.zeros((seqs, width), F32)
    for i in range(o_parts):
        arrive(1)
        total += jnp.dot(
            heads_out[:, i * o_rows:(i + 1) * o_rows],
            wo[i * o_rows:(i + 1) * o_rows, :],
            preferred_element_type=F32,
        )
    partial[...] = total
    own = lax.axis_index("tp") * row_count
    other = seqs - row_count - own
    keep_ref[...] = partial[pl.ds(pl.multiple_of(own, 8), row_count), :].astype(BF16)
    send_ref[...] = partial[pl.ds(pl.multiple_of(other, 8), row_count), :].astype(BF16)


def attention(tokens, norm_attn, w_query, w_key, w_value, w_out, attn_bias,
              cache_keys, cache_values, lengths, row_count):
    seqs, width = tokens.shape
    q_width = w_query.shape[1]
    kv_width = w_key.shape[1]
    heads = q_width // HEAD_DIM
    group = GROUP if seqs % GROUP == 0 else 1
    q_parts = split_of(width, 4)
    o_parts = split_of(q_width, 4)
    dma = pltpu.SemaphoreType.DMA
    half = jax.ShapeDtypeStruct((row_count, width), BF16)
    kv = jax.ShapeDtypeStruct((seqs, kv_width), BF16)
    return pl.pallas_call(
        functools.partial(attention_kernel, row_count, group, q_parts, o_parts),
        out_shape=(half, half, kv, kv),
        in_specs=[HBM] * 10,
        out_specs=(VMEM,) * 4,
        scratch_shapes=[
            pltpu.SMEM(lengths.shape, jnp.int32),
            pltpu.VMEM(tokens.shape, BF16),
            pltpu.VMEM((1, width), F32),
            pltpu.SMEM(attn_bias.shape, F32),
            pltpu.VMEM(w_query.shape, BF16),
            pltpu.VMEM(w_key.shape, BF16),
            pltpu.VMEM(w_value.shape, BF16),
            pltpu.VMEM(w_out.shape, BF16),
            pltpu.VMEM(cache_keys.shape, BF16),
            pltpu.VMEM(cache_values.shape, BF16),
            pltpu.VMEM((seqs * heads, LANES), F32),
            pltpu.VMEM((seqs * heads, LANES), F32),
            pltpu.VMEM((4 * LANES, 2 * LANES), BF16),
            pltpu.VMEM((seqs, width), F32),
            dma((6 + q_parts + o_parts + 2 * (seqs // group),)),
        ],
        compiler_params=pltpu.CompilerParams(vmem_limit_bytes=36 * 2**20),
        name="attention",
    )(*in_hbm(lengths, tokens, norm_attn.reshape(1, -1), attn_bias, w_query, w_key,
              w_value, w_out, cache_keys, cache_values))


def middle_kernel(row_count, tokens_ref, keep_ref, got_ref, gain_ref, mix_ref, routes_ref,
                  weights_ref, out_ref, middle_ref, wide):
    width = keep_ref.shape[1]
    wide[...] = tokens_ref[...].astype(F32)
    own = pl.multiple_of(lax.axis_index("tp") * row_count, 8)
    attn_sum = keep_ref[...].astype(F32) + got_ref[...].astype(F32)
    middle = (wide[pl.ds(own, row_count), :] + attn_sum).astype(BF16)
    middle_ref[...] = middle
    normed = normed_block(middle.astype(F32), gain_ref[...])
    out_ref[:, :width] = normed
    dot = jnp.sum(normed.astype(F32) * mix_ref[...].astype(F32), axis=-1, keepdims=True)
    gate = 1.0 / (1.0 + jnp.exp(-dot))
    coarse = gate.astype(BF16).astype(F32)
    lane = lax.broadcasted_iota(jnp.int32, (row_count, LANES), 1)
    extra = jnp.where(lane == EXPERTS, coarse, 0.0)
    extra = jnp.where(lane == EXPERTS + 1, gate - coarse, extra)
    for choice in range(routes_ref.shape[1]):
        extra += jnp.where(
            lane == routes_ref[:, choice:choice + 1],
            weights_ref[:, choice:choice + 1].astype(F32), 0.0,
        )
    out_ref[:, width:] = extra.astype(BF16)


def make_middle(tokens, keep, got, norm_ffn, dense_mix, routes, route_weights):
    row_count, width = keep.shape
    return pl.pallas_call(
        functools.partial(middle_kernel, row_count),
        out_shape=(
            jax.ShapeDtypeStruct((row_count, width + LANES), BF16),
            jax.ShapeDtypeStruct((row_count, width), BF16),
        ),
        in_specs=[VMEM] * 7,
        out_specs=(VMEM,) * 2,
        scratch_shapes=[pltpu.VMEM(tokens.shape, F32)],
        compiler_params=pltpu.CompilerParams(vmem_limit_bytes=4 * 2**20),
        name="middle",
    )(tokens, keep, got, norm_ffn.reshape(1, -1), dense_mix.reshape(1, -1), routes,
      route_weights)


def units_part(units):
    return pl.ds(pl.multiple_of(lax.axis_index("tp") * units, 8), units)


def fetch_kernel(plan, count, *refs):
    sems = refs[-1]
    copies = [
        pltpu.make_async_copy(source, target, sems.at[i])
        for i, (source, target) in enumerate(plan(refs[1:1 + count], refs[1 + count:-1]))
    ]
    for copy in copies:
        copy.start()
    for copy in copies:
        copy.wait()


def fetch(after, arrays, shapes, copies, plan):
    size = sum(2 * math.prod(shape) for shape in shapes)
    return pl.pallas_call(
        functools.partial(fetch_kernel, plan, len(arrays)),
        out_shape=tuple(pltpu.VMEM(shape, BF16) for shape in shapes),
        in_specs=[HBM] * (1 + len(arrays)),
        out_specs=(VMEM,) * len(shapes),
        scratch_shapes=[pltpu.SemaphoreType.DMA((copies,))],
        cost_estimate=pl.CostEstimate(
            flops=FETCH_FLOPS * size, bytes_accessed=size, transcendentals=0
        ),
        compiler_params=pltpu.CompilerParams(vmem_limit_bytes=2**20),
    )(after, *in_hbm(*arrays))


def wide_plan(first, count, gate_hbm, up_hbm, target):
    pairs = []
    for i in range(count):
        cols = pl.ds((first + i) * BLOCK, BLOCK)
        pairs.append((gate_hbm.at[:, cols], target.at[i, :, pl.ds(0, BLOCK)]))
        pairs.append((up_hbm.at[:, cols], target.at[i, :, pl.ds(BLOCK, BLOCK)]))
    return pairs


def fetch_weights(after, expert_gate, expert_up, expert_down, dense_gate_w, dense_up_w,
                  dense_down_w):
    width, units = expert_gate.shape
    blocks = units // BLOCK
    early = 1
    joined = units % BLOCK == 0 and blocks > early + LAST
    dense_units = dense_gate_w.shape[1] // lax.axis_size("tp")

    def first_plan(sources, targets):
        part = units_part(dense_units)
        pairs = [
            (sources[i].at[part], target)
            for i, target in enumerate((targets[0].at[0], targets[0].at[1], targets[1]))
        ]
        if joined:
            return pairs + wide_plan(0, early, sources[3], sources[4], targets[2])
        return pairs + [(sources[3], targets[2].at[0])]

    def second_plan(sources, targets):
        half = units // 2
        return [
            (sources[0].at[pl.ds(i * half, half)], targets[0].at[pl.ds(i * half, half)])
            for i in range(2)
        ]

    cut = blocks - LAST

    def third_plan(sources, targets):
        if joined:
            return wide_plan(early, cut - early, *sources, targets[0])
        return [(sources[1], targets[0].at[0])]

    dense, dense_down, first_wide = fetch(
        after[0],
        (dense_gate_w.T, dense_up_w.T, dense_down_w, expert_gate, expert_up),
        (
            (2, dense_units, width), (dense_units, width),
            (early, width, 2 * BLOCK) if joined else (1, width, units),
        ),
        3 + (2 * early if joined else 1), first_plan,
    )
    down, = fetch(after[1], (expert_down,), ((units, width),), 2, second_plan)
    wides = [first_wide]
    wides += fetch(
        after[2], (expert_gate, expert_up),
        ((cut - early, width, 2 * BLOCK) if joined else (1, width, units),),
        2 * (cut - early) if joined else 1, third_plan,
    )
    if joined:
        wides += fetch(
            after[3], (expert_gate, expert_up), ((LAST, width, 2 * BLOCK),),
            2 * LAST, lambda sources, targets: wide_plan(cut, LAST, *sources, targets[0]),
        )
    return (dense, down, dense_down, *wides)


def ffn_kernel(members, out_block, rows_ref, dense, down, dense_down, *refs):
    wides, (own_ref, other_ref, hidden_ref) = refs[:-3], refs[-3:]
    count, padded = rows_ref.shape
    width = padded - LANES
    units = down.shape[0]
    device = lax.axis_index("ep") * lax.axis_size("tp") + lax.axis_index("tp")
    expert = device // members
    extra = rows_ref[:, width:].astype(F32)
    lane = lax.broadcasted_iota(jnp.int32, extra.shape, 1)
    share = jnp.sum(jnp.where(lane == expert, extra, 0.0), axis=-1, keepdims=True)
    gated = (lane == EXPERTS) | (lane == EXPERTS + 1)
    mix = jnp.sum(jnp.where(gated, extra, 0.0), axis=-1, keepdims=True)

    def activate(gate, up, scale):
        return (gate / (1.0 + jnp.exp(-gate)) * up * scale).astype(BF16)

    rows = rows_ref[:, :width]
    if wides[0].shape[2] == units:
        gate, up = (jnp.dot(rows, wide[0], preferred_element_type=F32) for wide in wides)
        hidden_ref[...] = activate(gate, up, share)
    else:
        weights = [wide.at[i] for wide in wides for i in range(wide.shape[0])]
        for i, weight in enumerate(weights):
            both = jnp.dot(rows, weight[...], preferred_element_type=F32)
            hidden_ref[:, i * BLOCK:(i + 1) * BLOCK] = activate(
                both[:, :BLOCK], both[:, BLOCK:], share
            )
    dims = (((1,), (1,)), ((), ()))
    gate, up = (
        lax.dot_general(rows, dense[i], dims, preferred_element_type=F32) for i in range(2)
    )
    dense_hidden = activate(gate, up, mix)
    for first in range(0, width, out_block):
        cols = slice(first, first + out_block)
        total = jnp.dot(hidden_ref[...], down[:, cols], preferred_element_type=F32)
        total += jnp.dot(dense_hidden, dense_down[:, cols], preferred_element_type=F32)
        own_ref[:, cols] = total[:count // 2]
        other_ref[:, cols] = total[count // 2:].astype(BF16)


def feed_forward(rows, weights, members):
    count, padded = rows.shape
    width = padded - LANES
    units = weights[1].shape[0]
    return pl.pallas_call(
        functools.partial(ffn_kernel, members, 512 if width % 512 == 0 else width),
        out_shape=(
            jax.ShapeDtypeStruct((count // 2, width), F32),
            jax.ShapeDtypeStruct((count // 2, width), BF16),
        ),
        in_specs=[VMEM] * (1 + len(weights)),
        out_specs=(VMEM,) * 2,
        scratch_shapes=[pltpu.VMEM((count, units), BF16)],
        cost_estimate=pl.CostEstimate(
            flops=6 * count * width * units, bytes_accessed=0, transcendentals=0
        ),
        compiler_params=pltpu.CompilerParams(vmem_limit_bytes=16 * 2**20),
        name="feed_forward",
    )(rows, *weights)


def phases_of(n_ep):
    bits = [1 << b for b in range(n_ep.bit_length() - 1)]
    if len(bits) < 4:
        doublings = [(bit, bit) for bit in bits[2:]]
        direct = [(1, 2), (2, 1), (3, 3)] if len(bits) >= 2 else [(bit, bit) for bit in bits]
        return doublings, direct
    high, low = bits[-1], bits[-2]
    doublings = list(zip(bits[:1:-1], [2, 1] + bits[2:-2]))
    return doublings, [(2, high | low), (1, low), (3, high)]


def exchange(array, masks, n_ep, n_tp):
    pairs = [
        (ep * n_tp + tp, (ep ^ masks[tp % 2]) * n_tp + tp)
        for ep in range(n_ep) for tp in range(n_tp)
    ]
    return lax.ppermute(array, ("ep", "tp"), pairs)


def swap(array, n_tp):
    return lax.ppermute(array, "tp", [(i, i ^ 1) for i in range(n_tp)])


def layer(
    tokens, norm_attn, w_query, w_key, w_value, w_out, attn_bias, cache_keys, cache_values,
    lengths, norm_ffn, expert_gate, expert_up, expert_down, dense_gate_w, dense_up_w,
    dense_down_w, dense_mix, routes, route_weights,
):
    n_ep, n_tp = lax.axis_size("ep"), lax.axis_size("tp")
    row_count = tokens.shape[0] // n_tp
    keep, send, new_keys, new_values = attention(
        tokens, norm_attn, w_query, w_key, w_value, w_out, attn_bias, cache_keys,
        cache_values, lengths, row_count,
    )
    rows, middle = make_middle(
        tokens, keep, swap(send, n_tp), norm_ffn, dense_mix, routes, route_weights
    )
    doublings, direct = phases_of(n_ep)
    held = []
    for masks in doublings:
        held.append(rows)
        got = exchange(rows, masks, n_ep, n_tp)
        rows = jnp.concatenate([rows, got], axis=0)
    pieces = [rows]
    for masks in direct:
        pieces.append(exchange(rows, masks, n_ep, n_tp))
    rows = jnp.concatenate(pieces, axis=0)
    weights = fetch_weights(
        (held[-2], held[-1], pieces[0], rows), expert_gate, expert_up, expert_down, dense_gate_w,
        dense_up_w, dense_down_w,
    )
    got = swap(rows, n_tp)
    rows = jnp.concatenate([rows, got], axis=0)
    own, other = feed_forward(rows, weights, n_ep * n_tp // EXPERTS)
    total = own + swap(other, n_tp).astype(F32)
    part = total.shape[0] // (2 * (len(direct) + 1))
    sums = []
    for side in (1, 0):
        sent = [
            exchange(
                total[(2 * i + 2 + side) * part:(2 * i + 3 + side) * part].astype(BF16),
                masks, n_ep, n_tp,
            )
            for i, masks in enumerate(direct)
        ]
        summed = total[side * part:(side + 1) * part]
        for got in sent:
            summed = summed + got.astype(F32)
        sums.append(summed)
    second, total = sums
    got = exchange(second.astype(BF16), doublings[-1], n_ep, n_tp)
    total = total + got.astype(F32)
    for masks in reversed(doublings[:-1]):
        half = total.shape[0] // 2
        got = exchange(total[half:].astype(BF16), masks, n_ep, n_tp)
        total = total[:half] + got.astype(F32)
    layer_out = (middle.astype(F32) + total).astype(BF16)
    return layer_out, new_keys, new_values


def solution(mesh):
    placed = (
        P("ep", None),
        P(),
        P(None, "tp"),
        P(None, "tp"),
        P(None, "tp"),
        P("tp", None),
        P("tp"),
        P("ep", None, "tp"),
        P("ep", None, "tp"),
        P("ep"),
        P(),
        P(None, ("ep", "tp")),
        P(None, ("ep", "tp")),
        P(("ep", "tp"), None),
        P(None, "ep"),
        P(None, "ep"),
        P("ep", None),
        P(),
        P(("ep", "tp"), None),
        P(("ep", "tp"), None),
    )
    return jax.shard_map(
        layer,
        mesh=mesh,
        in_specs=placed,
        out_specs=(P(("ep", "tp"), None), P("ep", "tp"), P("ep", "tp")),
        check_vma=False,
    )
```
